512 devices in a mesh: dp: 4 (over x), kv: 64 (over z, y), tp: 2 (over core).
Axes of the slice: x: 4, y: 8, z: 8, core: 2. Of those that a mesh axis runs over, the one named last changes fastest.
Arguments:
- tokens: bfloat16 [512, 4096], P('dp', ('kv', 'tp')), may hold values from -6 to 6
- w_query: bfloat16 [4096, 2, 1024], P(None, 'tp', 'kv'), may hold values from -0.09375 to 0.09375
- w_forget: bfloat16 [4096, 2, 1024], P(None, 'tp', 'kv'), may hold values from -0.09375 to 0.09375
- w_input: bfloat16 [4096, 2, 1024], P(None, 'tp', 'kv'), may hold values from -0.09375 to 0.09375
- w_output_gate: bfloat16 [4096, 2, 1024], P(None, 'tp', 'kv'), may hold values from -0.09375 to 0.09375
- gate_floor: float32 [2048], P('tp'), may hold values from 0 to 0.9
- head_gain: float32 [128], replicated, may hold values from 0.1 to 1.9
- w_out: bfloat16 [2048, 4096], P(None, ('kv', 'tp')), may hold values from -0.125 to 0.125
- mix_gain: float32 [4096], replicated, may hold values from 0.1 to 1.9
- ffn_gain: float32 [4096], replicated, may hold values from 0.1 to 1.9
- w_up: bfloat16 [4096, 16384], P(None, ('kv', 'tp')), may hold values from -0.09375 to 0.09375
- w_down: bfloat16 [16384, 4096], P(('kv', 'tp')), may hold values from -0.1875 to 0.1875
- state: float32 [512, 16, 128, 128], P(('dp', 'kv'), 'tp'), may hold values from -6 to 6
Outputs:
- mixed: bfloat16 [512, 4096], P('dp', ('kv', 'tp'))
- new_state: float32 [512, 16, 128, 128], P(('dp', 'kv'), 'tp')
The draws below stay inside these ranges and needn't reach their ends.
All inputs are finite; a program needn't handle non-finite values.
Results may differ from the reference program's by a relative error of at most 0.014.
Values may be sent and summed in bfloat16 or wider, within the bound.
No kernel may reach another device: no remote copies, remote signals or barrier semaphores. Data moves between devices by JAX's collectives and lax.ppermute only.
A program may use at most 64 MiB of HBM per device.

```python
import jax
import jax.numpy as jnp
from jax import lax

D = 4096
HEADS = 16
HEAD = 128
FF = 16384
D_HG = 2048
BATCH = 512
N_TP = 2


def spiked(entries, stream_key, source, target, parts, factor):
    def block_of(position):
        return (jnp.arange(entries.shape[position]) // (entries.shape[position] // parts)).reshape((-1,) + (1,) * (entries.ndim - 1 - position))

    first = jax.random.permutation(stream_key, parts)[block_of(target)]
    second = (block_of(target) + parts // 2) % parts
    return jnp.where((block_of(source) == first) | (block_of(source) == second), factor * entries, entries)


def shard_levels(stream_key, shape, split, smallest, largest):
    def one(position, shards_of):
        heights = jax.random.uniform(jax.random.fold_in(jax.random.fold_in(stream_key, 6), position), (shards_of,), jnp.float32, smallest / len(split), largest / len(split))
        return jnp.repeat(jnp.exp(heights), shape[position] // shards_of).reshape((-1,) + (1,) * (len(shape) - position - 1))

    level = one(*split[0])
    for cut in split[1:]:
        level = level * one(*cut)
    return level


def gaussian(key, shape, scale, reach, cuts=(), held_as=jnp.bfloat16):
    drawn = scale * jax.random.normal(key, shape, jnp.float32)
    if cuts:
        drawn = drawn * shard_levels(key, shape, cuts, -0.22, 0.18)
    return jnp.clip(drawn, -reach, reach).astype(held_as)


def heavy_noise(rng, dims, deviation, limit, cuts, heavy, kind=jnp.bfloat16):
    result = deviation * jax.random.normal(rng, dims, jnp.float32)
    if cuts:
        result = result * shard_levels(rng, dims, cuts, -0.22, 0.18)
    return jnp.clip(spiked(result, jax.random.fold_in(rng, 3), *heavy), -limit, limit).astype(kind)


def setup_inputs(seed: int = 0) -> dict:
    key_of = jax.random.split(jax.random.key(seed), 14)
    return {
        "tokens": gaussian(key_of[0], (BATCH, D), 1.0, 6.0, ((0, 4), (1, 128))),
        "w_query": gaussian(key_of[1], (D, N_TP, D_HG // N_TP), D ** -0.5, 0.09375, ((1, 2), (2, 64))),
        "w_forget": gaussian(key_of[2], (D, N_TP, D_HG // N_TP), D ** -0.5, 0.09375, ((1, 2), (2, 64))),
        "w_input": gaussian(key_of[3], (D, N_TP, D_HG // N_TP), D ** -0.5, 0.09375, ((1, 2), (2, 64))),
        "w_output_gate": gaussian(key_of[4], (D, N_TP, D_HG // N_TP), D ** -0.5, 0.09375, ((1, 2), (2, 64))),
        "gate_floor": jnp.clip(0.9 * jax.random.uniform(key_of[5], (D_HG,), jnp.float32) ** shard_levels(key_of[5], (D_HG,), ((0, 2),), -0.2, 0.2), 0.0, 0.9),
        "head_gain": jnp.clip(1.0 + 0.18 * jax.random.normal(key_of[6], (HEAD,), jnp.float32), 0.1, 1.9),
        "w_out": gaussian(key_of[7], (D_HG, D), D_HG ** -0.5, 0.125, ((1, 128),)),
        "mix_gain": jnp.clip(1.0 + 0.18 * jax.random.normal(key_of[8], (D,), jnp.float32), 0.1, 1.9),
        "ffn_gain": jnp.clip(1.0 + 0.18 * jax.random.normal(key_of[9], (D,), jnp.float32), 0.1, 1.9),
        "w_up": gaussian(key_of[10], (D, FF), D ** -0.5, 0.09375, ((1, 128),)),
        "w_down": heavy_noise(key_of[11], (FF, D), FF ** -0.5, 0.1875, ((0, 128),), (0, 1, 128, 5.5)),
        "state": gaussian(key_of[12], (BATCH, HEADS, HEAD, HEAD), 1.0, 6.0, ((0, 256), (1, 2)), jnp.float32),
    }


EPSILON = 1e-06

def rms_scale(values, gain):
    return values * lax.rsqrt(lax.optimization_barrier(jnp.mean(values * values, axis=-1, keepdims=True)) + EPSILON) * gain

def reference(tokens, w_query, w_forget, w_input, w_output_gate, gate_floor, head_gain, w_out, mix_gain, ffn_gain, w_up, w_down, state):
    tokens_f = tokens.astype(jnp.float32)
    normed = rms_scale(tokens_f, mix_gain).astype(jnp.bfloat16)

    def project(weight):
        return jnp.dot(normed, weight.reshape(D, D_HG), preferred_element_type=jnp.float32).astype(jnp.bfloat16)
    batch_rows = tokens.shape[0]
    query_raw = project(w_query).astype(jnp.float32).reshape(batch_rows, HEADS, HEAD)
    forget_raw = project(w_forget).astype(jnp.float32).reshape(batch_rows, HEADS, HEAD)
    input_vec = project(w_input).astype(jnp.float32).reshape(batch_rows, HEADS, HEAD)
    gate_raw = project(w_output_gate).astype(jnp.float32).reshape(batch_rows, HEADS, HEAD)
    query_vec = query_raw * HEAD ** (-0.5)
    floor_heads = gate_floor.reshape(HEADS, HEAD)
    forget_gate = floor_heads + (1.0 - floor_heads) * jax.nn.sigmoid(forget_raw)
    new_state = forget_gate[..., None] * state + (1.0 - forget_gate)[..., None] * input_vec[:, :, None, :]
    head_out = jnp.einsum('bhk,bhkv->bhv', query_vec, new_state, precision=lax.Precision.HIGHEST)
    branch = rms_scale(head_out, head_gain) * jax.nn.silu(gate_raw)
    branch = branch.reshape(batch_rows, D_HG).astype(jnp.bfloat16)
    residual_one = (tokens_f + jnp.dot(branch, w_out, preferred_element_type=jnp.float32)).astype(jnp.bfloat16)
    residual_f = residual_one.astype(jnp.float32)
    ffn_in = rms_scale(residual_f, ffn_gain).astype(jnp.bfloat16)
    upward = jnp.dot(ffn_in, w_up, preferred_element_type=jnp.float32)
    hidden = jnp.square(jax.nn.relu(upward)).astype(jnp.bfloat16)
    mixed = (residual_f + jnp.dot(hidden, w_down, preferred_element_type=jnp.float32)).astype(jnp.bfloat16)
    return (mixed, new_state)
```

```python
import jax
import jax.numpy as jnp
from jax import lax
from jax.experimental import pallas as pl
from jax.experimental.pallas import tpu as pltpu
from jax.sharding import Mesh
from jax.sharding import PartitionSpec as P

KV = ("kv_0", "kv_1")
KV_TP = ("kv_0", "kv_1", "tp")
DP_KV = ("dp", "kv_0", "kv_1")


EPSILON = 1e-06


def rms_scale(values, gain):
    return values * lax.rsqrt(jnp.mean(values * values, axis=-1, keepdims=True) + EPSILON) * gain


def swapped(x):
    return lax.ppermute(x, "tp", [(0, 1), (1, 0)])


def gathered(x):
    chips = lax.axis_size(KV)
    return lax.all_to_all(jnp.broadcast_to(x[None], (chips, *x.shape)), KV, 0, 0, tiled=True)


def contracted(left, right, dims):
    return lax.dot_general(
        left, right, ((dims[:1], dims[1:]), ((), ())), preferred_element_type=jnp.float32
    )


def square_sums(x):
    values = x.astype(jnp.float32)
    return jnp.sum(values * values, axis=0, keepdims=True)


CHUNK = 256


def selection(core, share):
    source = lax.broadcasted_iota(jnp.int32, (CHUNK, CHUNK // 2), 0)
    target = lax.broadcasted_iota(jnp.int32, (CHUNK, CHUNK // 2), 1)
    wanted = (target // share) * (2 * share) + core * share + target % share
    return jnp.where(source == wanted, 1.0, 0.0).astype(jnp.bfloat16)


def split_mix_kernel(share, core_ref, query_ref, forget_ref, input_ref, gate_ref, gain_ref, mine_ref, other_ref):
    core = core_ref[0]
    for ref, index in ((mine_ref, core), (other_ref, 1 - core)):
        chosen = selection(index, share)
        for chunk in range(query_ref.shape[1] // CHUNK):
            span = pl.ds(chunk * CHUNK, CHUNK)
            block = jnp.concatenate(
                [
                    (part[:, span].astype(jnp.float32) * gain_ref[:, span]).astype(jnp.bfloat16)
                    for part in (query_ref, forget_ref, input_ref, gate_ref)
                ],
                axis=0,
            )
            ref[:, pl.ds(chunk * CHUNK // 2, CHUNK // 2)] = jnp.dot(
                block, chosen, preferred_element_type=jnp.float32
            ).astype(jnp.bfloat16)


def split_up_kernel(share, core_ref, weight_ref, gain_ref, mine_ref, other_ref):
    core = core_ref[0]
    for ref, index in ((mine_ref, core), (other_ref, 1 - core)):
        chosen = selection(index, share)
        for chunk in range(weight_ref.shape[0] // CHUNK):
            span = pl.ds(chunk * CHUNK, CHUNK)
            flipped = weight_ref[span, :].astype(jnp.float32).T * gain_ref[:, span]
            ref[:, pl.ds(chunk * CHUNK // 2, CHUNK // 2)] = jnp.dot(
                flipped.astype(jnp.bfloat16), chosen, preferred_element_type=jnp.float32
            ).astype(jnp.bfloat16)


def split_down_kernel(share, core_ref, weight_ref, mine_ref, other_ref):
    core = core_ref[0]
    for ref, index in ((mine_ref, core), (other_ref, 1 - core)):
        chosen = selection(index, share)
        for chunk in range(weight_ref.shape[1] // CHUNK):
            span = pl.ds(chunk * CHUNK, CHUNK)
            picked = jnp.dot(weight_ref[:, span], chosen, preferred_element_type=jnp.float32)
            ref[pl.ds(chunk * CHUNK // 2, CHUNK // 2), :] = picked.T.astype(jnp.bfloat16)


def split_call(kernel, share, shape, *operands):
    core = lax.axis_index("tp").astype(jnp.int32).reshape(1)
    memory = pl.BlockSpec(memory_space=pltpu.VMEM)
    return pl.pallas_call(
        lambda *refs: kernel(share, *refs),
        out_shape=[jax.ShapeDtypeStruct(shape, jnp.bfloat16)] * 2,
        in_specs=[pl.BlockSpec(memory_space=pltpu.SMEM)] + [memory] * len(operands),
        out_specs=[memory] * 2,
    )(core, *operands)


def per_device(
    tokens,
    w_query,
    w_forget,
    w_input,
    w_output_gate,
    gate_floor,
    head_gain,
    w_out,
    mix_gain,
    ffn_gain,
    w_up,
    w_down,
    state,
):
    chips = lax.axis_size(KV)
    cores = lax.axis_size("tp")
    rows, share = tokens.shape
    width = chips * cores * share
    seq_local, heads_local, head_size, _ = state.shape
    tokens_t = tokens.T
    columns = w_query.shape[2]
    hidden_local = w_up.shape[1]

    with jax.named_scope("gather_tokens"):
        token_half = gathered(tokens_t).reshape(chips * share, rows)
    with jax.named_scope("mix_weights"):
        mine, other = split_call(
            split_mix_kernel,
            share,
            (4 * columns, chips * share),
            *[w[:, 0, :].T for w in (w_query, w_forget, w_input, w_output_gate)],
            mix_gain[None, :],
        )
        lent = swapped(other)
    with jax.named_scope("project"):
        sums = square_sums(token_half)
        theirs = contracted(lent, token_half, (1, 0))
        arrived = swapped(jnp.concatenate([theirs, sums], axis=0))
        projected = contracted(mine, token_half, (1, 0)) + arrived[:-1]
        scale = lax.rsqrt((sums + arrived[-1:]) / width + EPSILON)
        raw = (projected * scale).astype(jnp.bfloat16).T
    with jax.named_scope("to_owner"):
        raw = lax.all_to_all(
            raw.reshape(chips, seq_local, 4 * columns), KV, split_axis=0, concat_axis=0, tiled=True
        )
        raw = raw.reshape(chips, seq_local, 4, columns).transpose(2, 1, 0, 3)
        raw = raw.reshape(4, seq_local, heads_local, head_size).astype(jnp.float32)

    query_vec = raw[0] * head_size ** (-0.5)
    floor_heads = gate_floor.reshape(heads_local, head_size)
    forget_gate = floor_heads + (1.0 - floor_heads) * jax.nn.sigmoid(raw[1])
    input_vec = raw[2]
    gate_vec = raw[3]
    new_state = (
        forget_gate[..., None] * state + (1.0 - forget_gate)[..., None] * input_vec[:, :, None, :]
    )
    head_out = jnp.einsum("bhk,bhkv->bhv", query_vec, new_state, precision=lax.Precision.HIGHEST)
    branch = rms_scale(head_out, head_gain) * jax.nn.silu(gate_vec)
    branch = branch.reshape(seq_local, heads_local * head_size).astype(jnp.bfloat16)

    with jax.named_scope("up_weights"):
        own_up, other = split_call(
            split_up_kernel, share, (hidden_local, chips * share), w_up, ffn_gain[None, :]
        )
        branch, own_up, lent_up = lax.optimization_barrier((branch, own_up, swapped(other)))

    with jax.named_scope("gather_branch"):
        branch_half = gathered(branch).reshape(rows, heads_local * head_size)
    with jax.named_scope("out_weights"):
        tp = lax.axis_index("tp")
        span = heads_local * head_size
        own_out = lax.dynamic_slice_in_dim(w_out, tp * span, span, 0)
        lent_out = swapped(lax.dynamic_slice_in_dim(w_out, (1 - tp) * span, span, 0))
    with jax.named_scope("out_product"):
        theirs = swapped(contracted(lent_out, branch_half, (0, 1)))
        projected = contracted(own_out, branch_half, (0, 1)) + theirs
        residual = (tokens_t.astype(jnp.float32) + projected).astype(jnp.bfloat16)

    with jax.named_scope("down_weights"):
        own_down, other = split_call(
            split_down_kernel, share, (chips * share, hidden_local), w_down
        )
        residual, own_down, lent_down = lax.optimization_barrier(
            (residual, own_down, swapped(other))
        )

    with jax.named_scope("gather_residual"):
        residual_half = gathered(residual).reshape(chips * share, rows)
    with jax.named_scope("up_product"):
        up_both = jnp.concatenate([own_up, lent_up], axis=0)
        partial = contracted(up_both, residual_half, (1, 0))
        sums = square_sums(residual_half)
        arrived = swapped(jnp.concatenate([partial, sums], axis=0))
        upward = partial + jnp.concatenate(
            [arrived[hidden_local : 2 * hidden_local], arrived[:hidden_local]], axis=0
        )
        scale = lax.rsqrt((sums + arrived[-1:]) / width + EPSILON)
        hidden = jnp.square(jax.nn.relu(upward * scale)).astype(jnp.bfloat16)

    with jax.named_scope("down_product"):
        down_both = jnp.concatenate([own_down, lent_down], axis=1)
        terms = contracted(down_both, hidden, (1, 0)).astype(jnp.bfloat16)
    with jax.named_scope("sum_terms"):
        terms = lax.all_to_all(
            terms.reshape(chips, share, rows), KV, split_axis=0, concat_axis=0, tiled=True
        )
        summed = terms.astype(jnp.float32).sum(axis=0)
        mixed = (residual.astype(jnp.float32) + summed).astype(jnp.bfloat16).T
    return (mixed, new_state)


def solution(mesh):
    torus = Mesh(
        mesh.devices.reshape(mesh.shape["dp"], 8, 8, mesh.shape["tp"]), ("dp", "kv_0", "kv_1", "tp")
    )
    placed = (
        P("dp", KV_TP),
        P(None, "tp", KV),
        P(None, "tp", KV),
        P(None, "tp", KV),
        P(None, "tp", KV),
        P("tp"),
        P(),
        P(None, KV_TP),
        P(),
        P(),
        P(None, KV_TP),
        P(KV_TP, None),
        P(DP_KV, "tp", None, None),
    )
    return jax.shard_map(
        per_device,
        mesh=torus,
        in_specs=placed,
        out_specs=(P("dp", KV_TP), P(DP_KV, "tp", None, None)),
        check_vma=False,
    )
```

```python
import jax
import jax.numpy as jnp
from jax import lax
from jax.experimental import pallas as pl
from jax.experimental.pallas import tpu as pltpu
from jax.sharding import Mesh
from jax.sharding import PartitionSpec as P


FAR = "kv_a"
QUAD = "kv_b"
NEAR = "kv_1"
KV = (FAR, QUAD, NEAR)
KV_TP = (*KV, "tp")
DP_KV = ("dp", *KV)


EPSILON = 1e-06


def rms_scale(values, gain):
    return values * lax.rsqrt(jnp.mean(values * values, axis=-1, keepdims=True) + EPSILON) * gain


def swapped(x):
    return lax.ppermute(x, "tp", [(0, 1), (1, 0)])


def crossed(x, bit):
    return lax.ppermute(x, QUAD, [(b, b ^ bit) for b in range(lax.axis_size(QUAD))])


def gathered(x, axes=KV):
    devices = lax.axis_size(axes)
    return lax.all_to_all(jnp.broadcast_to(x[None], (devices, *x.shape)), axes, 0, 0, tiled=True)


def contracted(left, right, dims):
    return lax.dot_general(
        left, right, ((dims[:1], dims[1:]), ((), ())), preferred_element_type=jnp.float32
    )


def square_sums(x):
    values = x.astype(jnp.float32)
    return jnp.sum(values * values, axis=0, keepdims=True)


CHUNK = 256


def selection(core, share):
    source = lax.broadcasted_iota(jnp.int32, (CHUNK, CHUNK // 2), 0)
    target = lax.broadcasted_iota(jnp.int32, (CHUNK, CHUNK // 2), 1)
    wanted = (target // share) * (2 * share) + core * share + target % share
    return jnp.where(source == wanted, 1.0, 0.0).astype(jnp.bfloat16)


def split_mix_kernel(share, core_ref, query_ref, forget_ref, input_ref, gate_ref, gain_ref, mine_ref, other_ref):
    core = core_ref[0]
    for ref, index in ((mine_ref, core), (other_ref, 1 - core)):
        chosen = selection(index, share)
        for chunk in range(query_ref.shape[1] // CHUNK):
            span = pl.ds(chunk * CHUNK, CHUNK)
            block = jnp.concatenate(
                [
                    (part[:, span].astype(jnp.float32) * gain_ref[:, span]).astype(jnp.bfloat16)
                    for part in (query_ref, forget_ref, input_ref, gate_ref)
                ],
                axis=0,
            )
            ref[:, pl.ds(chunk * CHUNK // 2, CHUNK // 2)] = jnp.dot(
                block, chosen, preferred_element_type=jnp.float32
            ).astype(jnp.bfloat16)


def split_up_kernel(
    share, far, quad, near, core_ref, weight_ref, mine_gain_ref, other_gain_ref, mine_ref, other_ref
):
    core = core_ref[0]
    group = quad * share
    sides = ((mine_ref, mine_gain_ref, core), (other_ref, other_gain_ref, 1 - core))
    for ref, gain_ref, index in sides:
        offset = pl.multiple_of(index * share, share)
        for a in range(far):
            for y in range(near):
                chips = [(a * quad + b) * near + y for b in range(quad)]
                rows = [pl.ds(chip * 2 * share + offset, share) for chip in chips]
                block = jnp.concatenate([weight_ref[span, :] for span in rows], axis=0)
                lanes = pl.ds((a * near + y) * group, group)
                scaled = block.astype(jnp.float32).T * gain_ref[:, lanes]
                ref[:, lanes] = scaled.astype(jnp.bfloat16)


def split_down_kernel(share, core_ref, weight_ref, mine_ref, other_ref):
    core = core_ref[0]
    for ref, index in ((mine_ref, core), (other_ref, 1 - core)):
        chosen = selection(index, share)
        for chunk in range(weight_ref.shape[1] // CHUNK):
            span = pl.ds(chunk * CHUNK, CHUNK)
            picked = jnp.dot(weight_ref[:, span], chosen, preferred_element_type=jnp.float32)
            ref[pl.ds(chunk * CHUNK // 2, CHUNK // 2), :] = picked.T.astype(jnp.bfloat16)


def split_call(kernel, sizes, shape, *operands):
    core = lax.axis_index("tp").astype(jnp.int32).reshape(1)
    memory = pl.BlockSpec(memory_space=pltpu.VMEM)
    return pl.pallas_call(
        lambda *refs: kernel(*sizes, *refs),
        out_shape=[jax.ShapeDtypeStruct(shape, jnp.bfloat16)] * 2,
        in_specs=[pl.BlockSpec(memory_space=pltpu.SMEM)] + [memory] * len(operands),
        out_specs=[memory] * 2,
    )(core, *operands)


def per_device(
    tokens,
    w_query,
    w_forget,
    w_input,
    w_output_gate,
    gate_floor,
    head_gain,
    w_out,
    mix_gain,
    ffn_gain,
    w_up,
    w_down,
    state,
):
    chips = lax.axis_size(KV)
    cores = lax.axis_size("tp")
    far = lax.axis_size(FAR)
    quad = lax.axis_size(QUAD)
    near = lax.axis_size(NEAR)
    rows, share = tokens.shape
    width = chips * cores * share
    seq_local, heads_local, head_size, _ = state.shape
    tokens_t = tokens.T
    columns = w_query.shape[2]
    hidden_local = w_up.shape[1]
    half = chips * share
    a = lax.axis_index(FAR)
    b = lax.axis_index(QUAD)
    y = lax.axis_index(NEAR)
    tp = lax.axis_index("tp")

    token_parts = gathered(tokens_t)
    token_half = token_parts.reshape(half, rows)
    mine, other = split_call(
        split_mix_kernel,
        (share,),
        (4 * columns, half),
        *[w[:, 0, :].T for w in (w_query, w_forget, w_input, w_output_gate)],
        mix_gain[None, :],
    )
    lent = swapped(other)
    pair = jnp.stack([w_out.T, crossed(w_out.T, 2)])
    pair = jnp.where(b & 2 == 2, pair[::-1], pair)
    four = jnp.stack([pair, crossed(pair, 1)], axis=1)
    four = jnp.where(b & 1 == 1, four[:, ::-1], four)
    out_columns = four.reshape(quad * share, cores * heads_local * head_size)
    mine, lent, out_columns = lax.optimization_barrier((mine, lent, out_columns))
    sums = square_sums(token_half)
    theirs = contracted(lent, token_half, (1, 0))
    arrived = swapped(jnp.concatenate([theirs, sums], axis=0))
    projected = contracted(mine, token_half, (1, 0)) + arrived[:-1]
    scale = lax.rsqrt((sums + arrived[-1:]) / width + EPSILON)
    raw = (projected * scale).astype(jnp.bfloat16).T
    raw, w_up, ffn_gain, token_parts = lax.optimization_barrier((raw, w_up, ffn_gain, token_parts))
    raw = lax.all_to_all(
        raw.reshape(chips, seq_local, 4 * columns), KV, split_axis=0, concat_axis=0, tiled=True
    )
    raw = raw.reshape(chips, seq_local, 4, columns).transpose(2, 1, 0, 3)
    raw = raw.reshape(4, seq_local, heads_local, head_size).astype(jnp.float32)
    gains = ffn_gain.reshape(far, quad, near, cores, share).transpose(3, 0, 2, 1, 4)
    gains = gains.reshape(cores, 1, half)
    gains = [lax.dynamic_index_in_dim(gains, core, 0, keepdims=False) for core in (tp, 1 - tp)]
    own_up, other = split_call(
        split_up_kernel, (share, far, quad, near), (hidden_local, half), w_up, *gains
    )
    lent_up = swapped(other)
    parts = token_parts.reshape(far, quad, near, share, far, quad, near * seq_local)
    parts = lax.dynamic_slice(
        parts,
        (a, 0, y, 0, 0, b, 0),
        (1, quad, 1, share, far, 1, near * seq_local),
    )
    block = parts.reshape(quad * share, far * near * seq_local).T.astype(jnp.float32)

    query_vec = raw[0] * head_size ** (-0.5)
    floor_heads = gate_floor.reshape(heads_local, head_size)
    forget_gate = floor_heads + (1.0 - floor_heads) * jax.nn.sigmoid(raw[1])
    input_vec = raw[2]
    gate_vec = raw[3]
    new_state = (
        forget_gate[..., None] * state + (1.0 - forget_gate)[..., None] * input_vec[:, :, None, :]
    )
    head_out = jnp.einsum("bhk,bhkv->bhv", query_vec, new_state, precision=lax.Precision.HIGHEST)
    branch = rms_scale(head_out, head_gain) * jax.nn.silu(gate_vec)
    branch = branch.reshape(seq_local, heads_local * head_size).astype(jnp.bfloat16)
    branch, own_up, lent_up, block, w_down = lax.optimization_barrier(
        (branch, own_up, lent_up, block, w_down)
    )

    branch = gathered(branch, (FAR, NEAR, "tp"))
    branch = branch.reshape(far * near, cores, seq_local, heads_local * head_size)
    branch = branch.transpose(0, 2, 1, 3).reshape(far * near * seq_local, -1)
    own_down, other = split_call(split_down_kernel, (share,), (half, hidden_local), w_down)
    lent_down = swapped(other)
    residual = (block + contracted(branch, out_columns, (1, 1))).astype(jnp.bfloat16)
    residual, own_down, lent_down = lax.optimization_barrier((residual, own_down, lent_down))

    parts = gathered(residual).reshape(
        far, quad, near, far, near * seq_local, quad * share
    )
    residual_half = parts.transpose(3, 1, 4, 0, 2, 5).reshape(rows, half)
    up_both = jnp.concatenate([own_up, lent_up], axis=0)
    partial = contracted(up_both, residual_half, (1, 1))
    values = residual_half.astype(jnp.float32)
    sums = jnp.sum(values * values, axis=1)[None, :]
    arrived = swapped(jnp.concatenate([partial, sums], axis=0))
    upward = partial + jnp.concatenate(
        [arrived[hidden_local : 2 * hidden_local], arrived[:hidden_local]], axis=0
    )
    scale = lax.rsqrt((sums + arrived[-1:]) / width + EPSILON)
    hidden = jnp.square(jax.nn.relu(upward * scale)).astype(jnp.bfloat16)

    down_both = jnp.concatenate([own_down, lent_down], axis=1)
    terms = contracted(down_both, hidden, (1, 0)).astype(jnp.bfloat16)
    terms = lax.all_to_all(
        terms.reshape(chips, share, rows), KV, split_axis=0, concat_axis=0, tiled=True
    )
    own = lax.dynamic_slice(residual_half, (0, ((a * near + y) * quad + b) * share), (rows, share))
    summed = terms.astype(jnp.float32).sum(axis=0)
    mixed = (own.astype(jnp.float32).T + summed).astype(jnp.bfloat16).T
    return (mixed, new_state)


def solution(mesh):
    torus = Mesh(
        mesh.devices.reshape(mesh.shape["dp"], 2, 4, 8, mesh.shape["tp"]), ("dp", *KV_TP)
    )
    placed = (
        P("dp", KV_TP),
        P(None, "tp", KV),
        P(None, "tp", KV),
        P(None, "tp", KV),
        P(None, "tp", KV),
        P("tp"),
        P(),
        P(None, KV_TP),
        P(),
        P(),
        P(None, KV_TP),
        P(KV_TP, None),
        P(DP_KV, "tp", None, None),
    )

    return jax.shard_map(
        per_device,
        mesh=torus,
        in_specs=placed,
        out_specs=(P("dp", KV_TP), P(DP_KV, "tp", None, None)),
        check_vma=False,
    )
```

```python
import jax
import jax.numpy as jnp
from jax import lax
from jax.experimental import pallas as pl
from jax.experimental.pallas import tpu as pltpu
from jax.sharding import Mesh
from jax.sharding import PartitionSpec as P


KV = ("kv_0", "kv_1")
KV_TP = ("kv_0", "kv_1", "tp")
DP_KV = ("dp", "kv_0", "kv_1")


EPSILON = 1e-06


def rms_scale(values, gain):
    return values * lax.rsqrt(jnp.mean(values * values, axis=-1, keepdims=True) + EPSILON) * gain


def swapped(x):
    return lax.ppermute(x, "tp", [(0, 1), (1, 0)])


def gathered(x):
    chips = lax.axis_size(KV)
    return lax.all_to_all(jnp.broadcast_to(x[None], (chips, *x.shape)), KV, 0, 0, tiled=True)


def contracted(left, right, dims):
    return lax.dot_general(
        left, right, ((dims[:1], dims[1:]), ((), ())), preferred_element_type=jnp.float32
    )


def square_sums(x):
    values = x.astype(jnp.float32)
    return jnp.sum(values * values, axis=0, keepdims=True)


CHUNK = 256


def selection(core, share):
    source = lax.broadcasted_iota(jnp.int32, (CHUNK, CHUNK // 2), 0)
    target = lax.broadcasted_iota(jnp.int32, (CHUNK, CHUNK // 2), 1)
    wanted = (target // share) * (2 * share) + core * share + target % share
    return jnp.where(source == wanted, 1.0, 0.0).astype(jnp.bfloat16)


def split_mix_kernel(share, core_ref, query_ref, forget_ref, input_ref, gate_ref, gain_ref, mine_ref, other_ref):
    core = core_ref[0]
    for ref, index in ((mine_ref, core), (other_ref, 1 - core)):
        chosen = selection(index, share)
        for chunk in range(query_ref.shape[1] // CHUNK):
            span = pl.ds(chunk * CHUNK, CHUNK)
            block = jnp.concatenate(
                [
                    (part[:, span].astype(jnp.float32) * gain_ref[:, span]).astype(jnp.bfloat16)
                    for part in (query_ref, forget_ref, input_ref, gate_ref)
                ],
                axis=0,
            )
            ref[:, pl.ds(chunk * CHUNK // 2, CHUNK // 2)] = jnp.dot(
                block, chosen, preferred_element_type=jnp.float32
            ).astype(jnp.bfloat16)


def split_up_kernel(share, core_ref, weight_ref, gain_ref, mine_ref, other_ref):
    core = core_ref[0]
    for ref, index in ((mine_ref, core), (other_ref, 1 - core)):
        chosen = selection(index, share)
        for chunk in range(weight_ref.shape[0] // CHUNK):
            span = pl.ds(chunk * CHUNK, CHUNK)
            flipped = weight_ref[span, :].astype(jnp.float32).T * gain_ref[:, span]
            ref[:, pl.ds(chunk * CHUNK // 2, CHUNK // 2)] = jnp.dot(
                flipped.astype(jnp.bfloat16), chosen, preferred_element_type=jnp.float32
            ).astype(jnp.bfloat16)


def split_down_kernel(share, core_ref, weight_ref, mine_ref, other_ref):
    core = core_ref[0]
    for ref, index in ((mine_ref, core), (other_ref, 1 - core)):
        chosen = selection(index, share)
        for chunk in range(weight_ref.shape[1] // CHUNK):
            span = pl.ds(chunk * CHUNK, CHUNK)
            picked = jnp.dot(weight_ref[:, span], chosen, preferred_element_type=jnp.float32)
            ref[pl.ds(chunk * CHUNK // 2, CHUNK // 2), :] = picked.T.astype(jnp.bfloat16)


def split_call(kernel, share, shape, *operands):
    core = lax.axis_index("tp").astype(jnp.int32).reshape(1)
    memory = pl.BlockSpec(memory_space=pltpu.VMEM)
    return pl.pallas_call(
        lambda *refs: kernel(share, *refs),
        out_shape=[jax.ShapeDtypeStruct(shape, jnp.bfloat16)] * 2,
        in_specs=[pl.BlockSpec(memory_space=pltpu.SMEM)] + [memory] * len(operands),
        out_specs=[memory] * 2,
    )(core, *operands)


def per_device(
    tokens,
    w_query,
    w_forget,
    w_input,
    w_output_gate,
    gate_floor,
    head_gain,
    w_out,
    mix_gain,
    ffn_gain,
    w_up,
    w_down,
    state,
):
    chips = lax.axis_size(KV)
    cores = lax.axis_size("tp")
    rows, share = tokens.shape
    width = chips * cores * share
    seq_local, heads_local, head_size, _ = state.shape
    tokens_t = tokens.T
    columns = w_query.shape[2]
    hidden_local = w_up.shape[1]

    token_half = gathered(tokens_t).reshape(chips * share, rows)
    mine, other = split_call(
        split_mix_kernel,
        share,
        (4 * columns, chips * share),
        *[w[:, 0, :].T for w in (w_query, w_forget, w_input, w_output_gate)],
        mix_gain[None, :],
    )
    lent = swapped(other)
    sums = square_sums(token_half)
    theirs = contracted(lent, token_half, (1, 0))
    arrived = swapped(jnp.concatenate([theirs, sums], axis=0))
    projected = contracted(mine, token_half, (1, 0)) + arrived[:-1]
    scale = lax.rsqrt((sums + arrived[-1:]) / width + EPSILON)
    raw = (projected * scale).astype(jnp.bfloat16).T
    raw = lax.all_to_all(
        raw.reshape(chips, seq_local, 4 * columns), KV, split_axis=0, concat_axis=0, tiled=True
    )
    raw = raw.reshape(chips, seq_local, 4, columns).transpose(2, 1, 0, 3)
    raw = raw.reshape(4, seq_local, heads_local, head_size).astype(jnp.float32)

    query_vec = raw[0] * head_size ** (-0.5)
    floor_heads = gate_floor.reshape(heads_local, head_size)
    forget_gate = floor_heads + (1.0 - floor_heads) * jax.nn.sigmoid(raw[1])
    input_vec = raw[2]
    gate_vec = raw[3]
    new_state = (
        forget_gate[..., None] * state + (1.0 - forget_gate)[..., None] * input_vec[:, :, None, :]
    )
    head_out = jnp.einsum("bhk,bhkv->bhv", query_vec, new_state, precision=lax.Precision.HIGHEST)
    branch = rms_scale(head_out, head_gain) * jax.nn.silu(gate_vec)
    branch = branch.reshape(seq_local, heads_local * head_size).astype(jnp.bfloat16)

    own_up, other = split_call(
        split_up_kernel, share, (hidden_local, chips * share), w_up, ffn_gain[None, :]
    )
    branch, own_up, lent_up = lax.optimization_barrier((branch, own_up, swapped(other)))

    branch_half = gathered(branch).reshape(rows, heads_local * head_size)
    tp = lax.axis_index("tp")
    span = heads_local * head_size
    own_out = lax.dynamic_slice_in_dim(w_out, tp * span, span, 0)
    lent_out = swapped(lax.dynamic_slice_in_dim(w_out, (1 - tp) * span, span, 0))
    theirs = swapped(contracted(lent_out, branch_half, (0, 1)))
    projected = contracted(own_out, branch_half, (0, 1)) + theirs
    residual = (tokens_t.astype(jnp.float32) + projected).astype(jnp.bfloat16)

    own_down, other = split_call(split_down_kernel, share, (chips * share, hidden_local), w_down)
    residual, own_down, lent_down = lax.optimization_barrier((residual, own_down, swapped(other)))

    residual_half = gathered(residual).reshape(chips * share, rows)
    up_both = jnp.concatenate([own_up, lent_up], axis=0)
    partial = contracted(up_both, residual_half, (1, 0))
    sums = square_sums(residual_half)
    arrived = swapped(jnp.concatenate([partial, sums], axis=0))
    upward = partial + jnp.concatenate(
        [arrived[hidden_local : 2 * hidden_local], arrived[:hidden_local]], axis=0
    )
    scale = lax.rsqrt((sums + arrived[-1:]) / width + EPSILON)
    hidden = jnp.square(jax.nn.relu(upward * scale)).astype(jnp.bfloat16)

    down_both = jnp.concatenate([own_down, lent_down], axis=1)
    terms = contracted(down_both, hidden, (1, 0)).astype(jnp.bfloat16)
    terms = lax.all_to_all(
        terms.reshape(chips, share, rows), KV, split_axis=0, concat_axis=0, tiled=True
    )
    summed = terms.astype(jnp.float32).sum(axis=0)
    mixed = (residual.astype(jnp.float32) + summed).astype(jnp.bfloat16).T
    return (mixed, new_state)


def solution(mesh):
    torus = Mesh(
        mesh.devices.reshape(mesh.shape["dp"], 8, 8, mesh.shape["tp"]), ("dp", "kv_0", "kv_1", "tp")
    )
    placed = (
        P("dp", KV_TP),
        P(None, "tp", KV),
        P(None, "tp", KV),
        P(None, "tp", KV),
        P(None, "tp", KV),
        P("tp"),
        P(),
        P(None, KV_TP),
        P(),
        P(),
        P(None, KV_TP),
        P(KV_TP, None),
        P(DP_KV, "tp", None, None),
    )

    return jax.shard_map(
        per_device,
        mesh=torus,
        in_specs=placed,
        out_specs=(P("dp", KV_TP), P(DP_KV, "tp", None, None)),
        check_vma=False,
    )
```

```python
import jax
import jax.numpy as jnp
from jax import lax
from jax.experimental import pallas as pl
from jax.experimental.pallas import tpu as pltpu
from jax.sharding import Mesh
from jax.sharding import PartitionSpec as P


KV = ("kv_0", "kv_1")
KV_TP = ("kv_0", "kv_1", "tp")
DP_KV = ("dp", "kv_0", "kv_1")


EPSILON = 1e-06


def rms_scale(values, gain):
    return values * lax.rsqrt(jnp.mean(values * values, axis=-1, keepdims=True) + EPSILON) * gain


def swapped(x):
    return lax.ppermute(x, "tp", [(0, 1), (1, 0)])


def gathered(x):
    chips = lax.axis_size(KV)
    return lax.all_to_all(jnp.broadcast_to(x[None], (chips, *x.shape)), KV, 0, 0, tiled=True)


def contracted(left, right, dims):
    return lax.dot_general(
        left, right, ((dims[:1], dims[1:]), ((), ())), preferred_element_type=jnp.float32
    )


def square_sums(x):
    values = x.astype(jnp.float32)
    return jnp.sum(values * values, axis=0, keepdims=True)


CHUNK = 256


def selection(core, share):
    source = lax.broadcasted_iota(jnp.int32, (CHUNK, CHUNK // 2), 0)
    target = lax.broadcasted_iota(jnp.int32, (CHUNK, CHUNK // 2), 1)
    wanted = (target // share) * (2 * share) + core * share + target % share
    return jnp.where(source == wanted, 1.0, 0.0).astype(jnp.bfloat16)


def split_mix_kernel(share, core_ref, query_ref, forget_ref, input_ref, gate_ref, gain_ref, mine_ref, other_ref):
    core = core_ref[0]
    for ref, index in ((mine_ref, core), (other_ref, 1 - core)):
        chosen = selection(index, share)
        for chunk in range(query_ref.shape[1] // CHUNK):
            span = pl.ds(chunk * CHUNK, CHUNK)
            block = jnp.concatenate(
                [
                    (part[:, span].astype(jnp.float32) * gain_ref[:, span]).astype(jnp.bfloat16)
                    for part in (query_ref, forget_ref, input_ref, gate_ref)
                ],
                axis=0,
            )
            ref[:, pl.ds(chunk * CHUNK // 2, CHUNK // 2)] = jnp.dot(
                block, chosen, preferred_element_type=jnp.float32
            ).astype(jnp.bfloat16)


def split_up_kernel(share, core_ref, weight_ref, gain_ref, mine_ref, other_ref):
    core = core_ref[0]
    for ref, index in ((mine_ref, core), (other_ref, 1 - core)):
        chosen = selection(index, share)
        for chunk in range(weight_ref.shape[0] // CHUNK):
            span = pl.ds(chunk * CHUNK, CHUNK)
            flipped = weight_ref[span, :].astype(jnp.float32).T * gain_ref[:, span]
            ref[:, pl.ds(chunk * CHUNK // 2, CHUNK // 2)] = jnp.dot(
                flipped.astype(jnp.bfloat16), chosen, preferred_element_type=jnp.float32
            ).astype(jnp.bfloat16)


def split_down_kernel(share, core_ref, weight_ref, mine_ref, other_ref):
    core = core_ref[0]
    for ref, index in ((mine_ref, core), (other_ref, 1 - core)):
        chosen = selection(index, share)
        for chunk in range(weight_ref.shape[1] // CHUNK):
            span = pl.ds(chunk * CHUNK, CHUNK)
            picked = jnp.dot(weight_ref[:, span], chosen, preferred_element_type=jnp.float32)
            ref[pl.ds(chunk * CHUNK // 2, CHUNK // 2), :] = picked.T.astype(jnp.bfloat16)


def project_kernel(mix_ref, tokens_ref, packed_ref):
    partial = jnp.dot(mix_ref[...], tokens_ref[...], preferred_element_type=jnp.float32)
    values = tokens_ref[...].astype(jnp.float32)
    sums = jnp.sum(values * values, axis=0, keepdims=True)
    high = sums.astype(jnp.bfloat16).astype(jnp.float32)
    cores, rows, lanes = packed_ref.shape
    columns = partial.shape[0] // cores
    place = lax.broadcasted_iota(jnp.int32, (lanes - columns, rows), 0)
    extra = jnp.where(place == 0, high, jnp.where(place == 1, sums - high, 0.0))
    for core in range(cores):
        block = jnp.concatenate([partial[core * columns : (core + 1) * columns], extra], axis=0)
        packed_ref[core] = block.T.astype(jnp.bfloat16)


def split_call(kernel, share, shape, *operands):
    core = lax.axis_index("tp").astype(jnp.int32).reshape(1)
    memory = pl.BlockSpec(memory_space=pltpu.VMEM)
    return pl.pallas_call(
        lambda *refs: kernel(share, *refs),
        out_shape=[jax.ShapeDtypeStruct(shape, jnp.bfloat16)] * 2,
        in_specs=[pl.BlockSpec(memory_space=pltpu.SMEM)] + [memory] * len(operands),
        out_specs=[memory] * 2,
    )(core, *operands)


def per_device(
    tokens,
    w_query,
    w_forget,
    w_input,
    w_output_gate,
    gate_floor,
    head_gain,
    w_out,
    mix_gain,
    ffn_gain,
    w_up,
    w_down,
    state,
):
    chips = lax.axis_size(KV)
    cores = lax.axis_size("tp")
    rows, share = tokens.shape
    width = chips * cores * share
    seq_local, heads_local, head_size, _ = state.shape
    tokens_t = tokens.T
    columns = w_query.shape[2]
    hidden_local = w_up.shape[1]

    tp = lax.axis_index("tp")

    token_half = gathered(tokens_t).reshape(chips * share, rows)
    mine, other = split_call(
        split_mix_kernel,
        share,
        (4 * columns, chips * share),
        *[w[:, 0, :].T for w in (w_query, w_forget, w_input, w_output_gate)],
        mix_gain[None, :],
    )
    lent = swapped(other)
    mix = jnp.concatenate([jnp.where(tp == 0, mine, lent), jnp.where(tp == 0, lent, mine)], axis=0)
    own_up, other = split_call(
        split_up_kernel, share, (hidden_local, chips * share), w_up, ffn_gain[None, :]
    )
    lent_up = swapped(other)
    mix, own_up, lent_up = lax.optimization_barrier((mix, own_up, lent_up))
    memory = pl.BlockSpec(memory_space=pltpu.VMEM)
    raw = pl.pallas_call(
        project_kernel,
        out_shape=jax.ShapeDtypeStruct((cores, rows, 128), jnp.bfloat16),
        in_specs=[memory] * 2,
        out_specs=memory,
    )(mix, token_half)
    raw = raw.reshape(cores, chips, seq_local, 128).transpose(1, 0, 2, 3)
    raw = raw.reshape(chips * cores, seq_local, 128)
    raw, w_out, w_down = lax.optimization_barrier((raw, w_out, w_down))
    raw = lax.all_to_all(raw, KV_TP, split_axis=0, concat_axis=0, tiled=True)
    raw = raw.reshape(chips, cores, seq_local, 128).astype(jnp.float32).sum(axis=1)
    sums = raw[0, :, 4 * columns : 4 * columns + 2].sum(axis=1)
    scale = lax.rsqrt(sums / width + EPSILON)
    raw = raw[:, :, : 4 * columns] * scale[None, :, None]
    raw = raw.reshape(chips, seq_local, 4, columns).transpose(2, 1, 0, 3)
    raw = raw.reshape(4, seq_local, heads_local, head_size)
    span = heads_local * head_size
    own_out = lax.dynamic_slice_in_dim(w_out, tp * span, span, 0)
    lent_out = swapped(lax.dynamic_slice_in_dim(w_out, (1 - tp) * span, span, 0))
    own_down, other = split_call(split_down_kernel, share, (chips * share, hidden_local), w_down)
    lent_down = swapped(other)

    query_vec = raw[0] * head_size ** (-0.5)
    floor_heads = gate_floor.reshape(heads_local, head_size)
    forget_gate = floor_heads + (1.0 - floor_heads) * jax.nn.sigmoid(raw[1])
    input_vec = raw[2]
    gate_vec = raw[3]
    new_state = (
        forget_gate[..., None] * state + (1.0 - forget_gate)[..., None] * input_vec[:, :, None, :]
    )
    head_out = jnp.einsum("bhk,bhkv->bhv", query_vec, new_state, precision=lax.Precision.HIGHEST)
    branch = rms_scale(head_out, head_gain) * jax.nn.silu(gate_vec)
    branch = branch.reshape(seq_local, heads_local * head_size).astype(jnp.bfloat16)

    branch, own_out, lent_out, own_down, lent_down = lax.optimization_barrier(
        (branch, own_out, lent_out, own_down, lent_down)
    )

    branch_half = gathered(branch).reshape(rows, heads_local * head_size)
    theirs = swapped(contracted(lent_out, branch_half, (0, 1)))
    projected = contracted(own_out, branch_half, (0, 1)) + theirs
    residual = (tokens_t.astype(jnp.float32) + projected).astype(jnp.bfloat16)

    residual_half = gathered(residual).reshape(chips * share, rows)
    up_both = jnp.concatenate([own_up, lent_up], axis=0)
    partial = contracted(up_both, residual_half, (1, 0))
    sums = square_sums(residual_half)
    arrived = swapped(jnp.concatenate([partial, sums], axis=0))
    upward = partial + jnp.concatenate(
        [arrived[hidden_local : 2 * hidden_local], arrived[:hidden_local]], axis=0
    )
    scale = lax.rsqrt((sums + arrived[-1:]) / width + EPSILON)
    hidden = jnp.square(jax.nn.relu(upward * scale)).astype(jnp.bfloat16)

    down_both = jnp.concatenate([own_down, lent_down], axis=1)
    terms = contracted(down_both, hidden, (1, 0)).astype(jnp.bfloat16)
    terms = lax.all_to_all(
        terms.reshape(chips, share, rows), KV, split_axis=0, concat_axis=0, tiled=True
    )
    summed = terms.astype(jnp.float32).sum(axis=0)
    mixed = (residual.astype(jnp.float32) + summed).astype(jnp.bfloat16).T
    return (mixed, new_state)


def solution(mesh):
    torus = Mesh(
        mesh.devices.reshape(mesh.shape["dp"], 8, 8, mesh.shape["tp"]), ("dp", "kv_0", "kv_1", "tp")
    )
    placed = (
        P("dp", KV_TP),
        P(None, "tp", KV),
        P(None, "tp", KV),
        P(None, "tp", KV),
        P(None, "tp", KV),
        P("tp"),
        P(),
        P(None, KV_TP),
        P(),
        P(),
        P(None, KV_TP),
        P(KV_TP, None),
        P(DP_KV, "tp", None, None),
    )

    return jax.shard_map(
        per_device,
        mesh=torus,
        in_specs=placed,
        out_specs=(P("dp", KV_TP), P(DP_KV, "tp", None, None)),
        check_vma=False,
    )
```

```python
import jax
import jax.numpy as jnp
from jax import lax
from jax.experimental import pallas as pl
from jax.experimental.pallas import tpu as pltpu
from jax.sharding import Mesh
from jax.sharding import PartitionSpec as P


KV = ("kv_0", "kv_1")
KV_TP = ("kv_0", "kv_1", "tp")
DP_KV = ("dp", "kv_0", "kv_1")


EPSILON = 1e-06


def rms_scale(values, gain):
    return values * lax.rsqrt(jnp.mean(values * values, axis=-1, keepdims=True) + EPSILON) * gain


def swapped(x):
    return lax.ppermute(x, "tp", [(0, 1), (1, 0)])


def gathered(x):
    chips = lax.axis_size(KV)
    return lax.all_to_all(jnp.broadcast_to(x[None], (chips, *x.shape)), KV, 0, 0, tiled=True)


def contracted(left, right, dims):
    return lax.dot_general(
        left, right, ((dims[:1], dims[1:]), ((), ())), preferred_element_type=jnp.float32
    )


def square_sums(x):
    values = x.astype(jnp.float32)
    return jnp.sum(values * values, axis=0, keepdims=True)


CHUNK = 256


def selection(core, share):
    source = lax.broadcasted_iota(jnp.int32, (CHUNK, CHUNK // 2), 0)
    target = lax.broadcasted_iota(jnp.int32, (CHUNK, CHUNK // 2), 1)
    wanted = (target // share) * (2 * share) + core * share + target % share
    return jnp.where(source == wanted, 1.0, 0.0).astype(jnp.bfloat16)


def split_kernel(
    share,
    core_ref,
    query_ref,
    forget_ref,
    input_ref,
    gate_ref,
    out_ref,
    up_ref,
    down_ref,
    mix_gain_ref,
    ffn_gain_ref,
    mine_ref,
    other_ref,
):
    core = core_ref[0]
    half = CHUNK // 2
    columns = query_ref.shape[0]
    hidden = down_ref.shape[0]
    span = out_ref.shape[1] // 2
    lines = out_ref.shape[0] // 2
    for ref, index in ((mine_ref, core), (other_ref, 1 - core)):
        chosen = selection(index, share)
        for chunk in range(up_ref.shape[0] // CHUNK):
            source = pl.ds(chunk * CHUNK, CHUNK)
            parts = [
                part[:, source].astype(jnp.float32) * mix_gain_ref[:, source]
                for part in (query_ref, forget_ref, input_ref, gate_ref)
            ]
            parts.append(up_ref[source, :].astype(jnp.float32).T * ffn_gain_ref[:, source])
            rows = jnp.concatenate([part.astype(jnp.bfloat16) for part in parts], axis=0)
            rows = jnp.concatenate([rows, down_ref[:, source]], axis=0)
            ref[: 4 * columns + 2 * hidden, pl.ds(chunk * half, half)] = jnp.dot(
                rows, chosen, preferred_element_type=jnp.float32
            ).astype(jnp.bfloat16)
        start = pl.multiple_of(index * span, span)
        for piece in range(2):
            ref[4 * columns + 2 * hidden :, pl.ds(piece * span, span)] = out_ref[
                pl.ds(piece * lines, lines), pl.ds(start, span)
            ]


def split_weights(share, *operands):
    columns, hidden = operands[0].shape[0], operands[6].shape[0]
    lines, width = operands[4].shape[0] // 2, operands[0].shape[1] // 2
    core = lax.axis_index("tp").astype(jnp.int32).reshape(1)
    memory = pl.BlockSpec(memory_space=pltpu.VMEM)
    shape = jax.ShapeDtypeStruct((4 * columns + 2 * hidden + lines, width), jnp.bfloat16)
    return pl.pallas_call(
        lambda *refs: split_kernel(share, *refs),
        out_shape=[shape] * 2,
        in_specs=[pl.BlockSpec(memory_space=pltpu.SMEM)] + [memory] * len(operands),
        out_specs=[memory] * 2,
    )(core, *operands)


def per_device(
    tokens,
    w_query,
    w_forget,
    w_input,
    w_output_gate,
    gate_floor,
    head_gain,
    w_out,
    mix_gain,
    ffn_gain,
    w_up,
    w_down,
    state,
):
    chips = lax.axis_size(KV)
    cores = lax.axis_size("tp")
    rows, share = tokens.shape
    width = chips * cores * share
    seq_local, heads_local, head_size, _ = state.shape
    tokens_t = tokens.T
    columns = w_query.shape[2]
    hidden_local = w_up.shape[1]

    tp = lax.axis_index("tp")

    token_half = gathered(tokens_t).reshape(chips * share, rows)
    mine, other = split_weights(
        share,
        *[w[:, 0, :].T for w in (w_query, w_forget, w_input, w_output_gate)],
        w_out.T,
        w_up,
        w_down,
        mix_gain[None, :],
        ffn_gain[None, :],
    )
    mine, lent = lax.optimization_barrier((mine, swapped(other)))
    cuts = (0, 4 * columns, 4 * columns + hidden_local, 4 * columns + 2 * hidden_local)
    (own_down, lent_down), (own_out, lent_out) = [
        [both[start:end] for both in (mine, lent)]
        for start, end in zip(cuts[2:], (cuts[3], mine.shape[0]))
    ]
    own_out, lent_out = [
        jnp.concatenate([both[:, : both.shape[1] // 2], both[:, both.shape[1] // 2 :]], axis=0)
        for both in (own_out, lent_out)
    ]
    down_both = jnp.concatenate([own_down, lent_down], axis=0)
    mine, lent, own_out, lent_out, down_both = lax.optimization_barrier(
        (mine, lent, own_out, lent_out, down_both)
    )
    (own_mix, lent_mix), (own_up, lent_up) = [
        [both[start:end] for both in (mine, lent)] for start, end in zip(cuts[:2], cuts[1:3])
    ]
    sums = square_sums(token_half)
    high = sums.astype(jnp.bfloat16).astype(jnp.float32)
    place = lax.broadcasted_iota(jnp.int32, (128 - 4 * columns, rows), 0)
    extra = jnp.where(place == 0, high, jnp.where(place == 1, sums - high, 0.0))
    own = contracted(own_mix, token_half, (1, 0))
    theirs = contracted(lent_mix, token_half, (1, 0))
    first, second = jnp.where(tp == 0, own, theirs), jnp.where(tp == 0, theirs, own)
    raw = jnp.stack(
        [jnp.concatenate([part, extra], axis=0).T for part in (first, second)]
    ).astype(jnp.bfloat16)
    raw = raw.reshape(cores * chips, seq_local, 128)
    raw = lax.all_to_all(raw, ("tp", *KV), split_axis=0, concat_axis=0, tiled=True)
    raw = raw.reshape(cores, chips, seq_local, 128).astype(jnp.float32).sum(axis=0)
    sums = raw[0, :, 4 * columns : 4 * columns + 2].sum(axis=1)
    scale = lax.rsqrt(sums / width + EPSILON)
    raw = raw[:, :, : 4 * columns] * scale[None, :, None]
    raw = raw.reshape(chips, seq_local, 4, columns).transpose(2, 1, 0, 3)
    raw = raw.reshape(4, seq_local, heads_local, head_size)
    query_vec = raw[0] * head_size ** (-0.5)
    floor_heads = gate_floor.reshape(heads_local, head_size)
    forget_gate = floor_heads + (1.0 - floor_heads) * jax.nn.sigmoid(raw[1])
    input_vec = raw[2]
    gate_vec = raw[3]
    new_state = (
        forget_gate[..., None] * state + (1.0 - forget_gate)[..., None] * input_vec[:, :, None, :]
    )
    head_out = jnp.einsum("bhk,bhkv->bhv", query_vec, new_state, precision=lax.Precision.HIGHEST)
    branch = rms_scale(head_out, head_gain) * jax.nn.silu(gate_vec)
    branch = branch.reshape(seq_local, heads_local * head_size).astype(jnp.bfloat16)

    branch_half = gathered(branch).reshape(rows, heads_local * head_size)
    theirs = swapped(contracted(lent_out, branch_half, (1, 1)))
    projected = contracted(own_out, branch_half, (1, 1)) + theirs
    residual = (tokens_t.astype(jnp.float32) + projected).astype(jnp.bfloat16)

    residual_half = gathered(residual).reshape(chips * share, rows)
    partial = jnp.concatenate(
        [contracted(up, residual_half, (1, 0)) for up in (own_up, lent_up)], axis=0
    )
    sums = square_sums(residual_half)
    arrived = swapped(jnp.concatenate([partial, sums], axis=0))
    upward = partial + jnp.concatenate(
        [arrived[hidden_local : 2 * hidden_local], arrived[:hidden_local]], axis=0
    )
    scale = lax.rsqrt((sums + arrived[-1:]) / width + EPSILON)
    hidden = jnp.square(jax.nn.relu(upward * scale)).astype(jnp.bfloat16)

    terms = contracted(down_both, hidden, (0, 0)).astype(jnp.bfloat16)
    terms = lax.all_to_all(
        terms.reshape(chips, share, rows), KV, split_axis=0, concat_axis=0, tiled=True
    )
    summed = terms.astype(jnp.float32).sum(axis=0)
    mixed = (residual.astype(jnp.float32) + summed).astype(jnp.bfloat16).T
    return (mixed, new_state)


def solution(mesh):
    torus = Mesh(
        mesh.devices.reshape(mesh.shape["dp"], 8, 8, mesh.shape["tp"]), ("dp", "kv_0", "kv_1", "tp")
    )
    placed = (
        P("dp", KV_TP),
        P(None, "tp", KV),
        P(None, "tp", KV),
        P(None, "tp", KV),
        P(None, "tp", KV),
        P("tp"),
        P(),
        P(None, KV_TP),
        P(),
        P(),
        P(None, KV_TP),
        P(KV_TP, None),
        P(DP_KV, "tp", None, None),
    )

    return jax.shard_map(
        per_device,
        mesh=torus,
        in_specs=placed,
        out_specs=(P("dp", KV_TP), P(DP_KV, "tp", None, None)),
        check_vma=False,
    )
```

```python
import jax
import jax.numpy as jnp
from jax import lax
from jax.experimental import pallas as pl
from jax.experimental.pallas import tpu as pltpu
from jax.sharding import Mesh
from jax.sharding import PartitionSpec as P


KV = ("kv_0", "kv_1")
KV_TP = ("kv_0", "kv_1", "tp")
DP_KV = ("dp", "kv_0", "kv_1")


EPSILON = 1e-06


def rms_scale(values, gain):
    return values * lax.rsqrt(jnp.mean(values * values, axis=-1, keepdims=True) + EPSILON) * gain


def swapped(x):
    return lax.ppermute(x, "tp", [(0, 1), (1, 0)])


def gathered(x):
    chips = lax.axis_size(KV)
    return lax.all_to_all(jnp.broadcast_to(x[None], (chips, *x.shape)), KV, 0, 0, tiled=True)


def contracted(left, right, dims):
    return lax.dot_general(
        left, right, ((dims[:1], dims[1:]), ((), ())), preferred_element_type=jnp.float32
    )


def square_sums(x):
    values = x.astype(jnp.float32)
    return jnp.sum(values * values, axis=0, keepdims=True)


CHUNK = 256


def selection(core, share):
    source = lax.broadcasted_iota(jnp.int32, (CHUNK, CHUNK // 2), 0)
    target = lax.broadcasted_iota(jnp.int32, (CHUNK, CHUNK // 2), 1)
    wanted = (target // share) * (2 * share) + core * share + target % share
    return jnp.where(source == wanted, 1.0, 0.0).astype(jnp.bfloat16)


def split_kernel(
    share,
    core_ref,
    query_ref,
    forget_ref,
    input_ref,
    gate_ref,
    out_ref,
    up_ref,
    down_ref,
    mix_gain_ref,
    ffn_gain_ref,
    mix_ref,
    own_up_ref,
    own_down_ref,
    own_out_ref,
    other_ref,
):
    core = core_ref[0]
    half = CHUNK // 2
    columns = query_ref.shape[0]
    hidden = down_ref.shape[0]
    span = out_ref.shape[1] // 2
    lines = out_ref.shape[0] // 2
    first, second = 4 * columns, 4 * columns + hidden
    for own, index in ((True, core), (False, 1 - core)):
        chosen = selection(index, share)
        for chunk in range(up_ref.shape[0] // CHUNK):
            source = pl.ds(chunk * CHUNK, CHUNK)
            target = pl.ds(chunk * half, half)
            parts = [
                part[:, source].astype(jnp.float32) * mix_gain_ref[:, source]
                for part in (query_ref, forget_ref, input_ref, gate_ref)
            ]
            parts.append(up_ref[source, :].astype(jnp.float32).T * ffn_gain_ref[:, source])
            rows = jnp.concatenate([part.astype(jnp.bfloat16) for part in parts], axis=0)
            rows = jnp.concatenate([rows, down_ref[:, source]], axis=0)
            picked = jnp.dot(rows, chosen, preferred_element_type=jnp.float32)
            picked = picked.astype(jnp.bfloat16)
            if own:
                mix_ref[:, target] = picked[:first]
                own_up_ref[:, target] = picked[first:second]
                own_down_ref[:, target] = picked[second:]
            else:
                other_ref[: second + hidden, target] = picked
        start = pl.multiple_of(index * span, span)
        if own:
            own_out_ref[...] = out_ref[:, pl.ds(start, span)]
        else:
            for piece in range(2):
                other_ref[second + hidden :, pl.ds(piece * span, span)] = out_ref[
                    pl.ds(piece * lines, lines), pl.ds(start, span)
                ]


def split_weights(share, *operands):
    columns, hidden = operands[0].shape[0], operands[6].shape[0]
    lines, width = operands[4].shape[0], operands[0].shape[1] // 2
    core = lax.axis_index("tp").astype(jnp.int32).reshape(1)
    memory = pl.BlockSpec(memory_space=pltpu.VMEM)
    shapes = (
        (4 * columns, width),
        (hidden, width),
        (hidden, width),
        (lines, operands[4].shape[1] // 2),
        (4 * columns + 2 * hidden + lines // 2, width),
    )
    return pl.pallas_call(
        lambda *refs: split_kernel(share, *refs),
        out_shape=[jax.ShapeDtypeStruct(shape, jnp.bfloat16) for shape in shapes],
        in_specs=[pl.BlockSpec(memory_space=pltpu.SMEM)] + [memory] * len(operands),
        out_specs=[memory] * len(shapes),
    )(core, *operands)


def per_device(
    tokens,
    w_query,
    w_forget,
    w_input,
    w_output_gate,
    gate_floor,
    head_gain,
    w_out,
    mix_gain,
    ffn_gain,
    w_up,
    w_down,
    state,
):
    chips = lax.axis_size(KV)
    cores = lax.axis_size("tp")
    rows, share = tokens.shape
    width = chips * cores * share
    seq_local, heads_local, head_size, _ = state.shape
    tokens_t = tokens.T
    columns = w_query.shape[2]
    hidden_local = w_up.shape[1]

    tp = lax.axis_index("tp")

    token_half = gathered(tokens_t).reshape(chips * share, rows)
    own_mix, own_up, own_down, own_out, other = split_weights(
        share,
        *[w[:, 0, :].T for w in (w_query, w_forget, w_input, w_output_gate)],
        w_out.T,
        w_up,
        w_down,
        mix_gain[None, :],
        ffn_gain[None, :],
    )
    lent = swapped(other)
    first = 4 * columns
    second, third = first + hidden_local, first + 2 * hidden_local
    span = lent.shape[1] // 2
    lent_out = jnp.concatenate([lent[third:, :span], lent[third:, span:]], axis=0)
    up_both = jnp.concatenate([own_up, lent[first:second]], axis=0)
    down_both = jnp.concatenate([own_down, lent[second:third]], axis=0)
    lent_mix, own_mix, own_out, lent_out, up_both, down_both = lax.optimization_barrier(
        (lent[:first], own_mix, own_out, lent_out, up_both, down_both)
    )
    sums = square_sums(token_half)
    high = sums.astype(jnp.bfloat16).astype(jnp.float32)
    place = lax.broadcasted_iota(jnp.int32, (128 - 4 * columns, rows), 0)
    extra = jnp.where(place == 0, high, jnp.where(place == 1, sums - high, 0.0))
    own = contracted(own_mix, token_half, (1, 0))
    theirs = contracted(lent_mix, token_half, (1, 0))
    first, second = jnp.where(tp == 0, own, theirs), jnp.where(tp == 0, theirs, own)
    raw = jnp.stack(
        [jnp.concatenate([part, extra], axis=0).T for part in (first, second)]
    ).astype(jnp.bfloat16)
    raw = raw.reshape(cores * chips, seq_local, 128)
    raw = lax.all_to_all(raw, ("tp", *KV), split_axis=0, concat_axis=0, tiled=True)
    raw, gate_floor, head_gain = lax.optimization_barrier((raw, gate_floor, head_gain))
    raw = raw.reshape(cores, chips, seq_local, 128).astype(jnp.float32).sum(axis=0)
    sums = raw[0, :, 4 * columns : 4 * columns + 2].sum(axis=1)
    scale = lax.rsqrt(sums / width + EPSILON)
    raw = raw[:, :, : 4 * columns] * scale[None, :, None]
    raw = raw.reshape(chips, seq_local, 4, columns).transpose(2, 1, 0, 3)
    raw = raw.reshape(4, seq_local, heads_local, head_size)
    query_vec = raw[0] * head_size ** (-0.5)
    floor_heads = gate_floor.reshape(heads_local, head_size)
    forget_gate = floor_heads + (1.0 - floor_heads) * jax.nn.sigmoid(raw[1])
    input_vec = raw[2]
    gate_vec = raw[3]
    new_state = (
        forget_gate[..., None] * state + (1.0 - forget_gate)[..., None] * input_vec[:, :, None, :]
    )
    head_out = jnp.sum(query_vec[..., None] * new_state, axis=2)
    branch = rms_scale(head_out, head_gain) * jax.nn.silu(gate_vec)
    branch = branch.reshape(seq_local, heads_local * head_size).astype(jnp.bfloat16)

    branch_half = gathered(branch).reshape(rows, heads_local * head_size)
    theirs = swapped(contracted(lent_out, branch_half, (1, 1)))
    projected = contracted(own_out, branch_half, (1, 1)) + theirs
    residual = (tokens_t.astype(jnp.float32) + projected).astype(jnp.bfloat16)

    residual_half = gathered(residual).reshape(chips * share, rows)
    partial = contracted(up_both, residual_half, (1, 0))
    sums = square_sums(residual_half)
    arrived = swapped(jnp.concatenate([partial, sums], axis=0))
    upward = partial + jnp.concatenate(
        [arrived[hidden_local : 2 * hidden_local], arrived[:hidden_local]], axis=0
    )
    scale = lax.rsqrt((sums + arrived[-1:]) / width + EPSILON)
    hidden = jnp.square(jax.nn.relu(upward * scale)).astype(jnp.bfloat16)

    terms = contracted(down_both, hidden, (0, 0)).astype(jnp.bfloat16)
    terms = lax.all_to_all(
        terms.reshape(chips, share, rows), KV, split_axis=0, concat_axis=0, tiled=True
    )
    summed = terms.astype(jnp.float32).sum(axis=0)
    mixed = (residual.astype(jnp.float32) + summed).astype(jnp.bfloat16).T
    return (mixed, new_state)


def solution(mesh):
    torus = Mesh(
        mesh.devices.reshape(mesh.shape["dp"], 8, 8, mesh.shape["tp"]), ("dp", "kv_0", "kv_1", "tp")
    )
    placed = (
        P("dp", KV_TP),
        P(None, "tp", KV),
        P(None, "tp", KV),
        P(None, "tp", KV),
        P(None, "tp", KV),
        P("tp"),
        P(),
        P(None, KV_TP),
        P(),
        P(),
        P(None, KV_TP),
        P(KV_TP, None),
        P(DP_KV, "tp", None, None),
    )

    return jax.shard_map(
        per_device,
        mesh=torus,
        in_specs=placed,
        out_specs=(P("dp", KV_TP), P(DP_KV, "tp", None, None)),
        check_vma=False,
    )
```

```python
import jax
import jax.numpy as jnp
from jax import lax
from jax.experimental import pallas as pl
from jax.experimental.pallas import tpu as pltpu
from jax.sharding import Mesh
from jax.sharding import PartitionSpec as P


KV = ("kv_far", "kv_pair", "kv_near")
PAIR = "kv_pair"
SIDE = ("kv_far", "kv_near")
KV_TP = (*KV, "tp")
DP_KV = ("dp", *KV)


EPSILON = 1e-06


def rms_scale(values, gain):
    return values * lax.rsqrt(jnp.mean(values * values, axis=-1, keepdims=True) + EPSILON) * gain


def swapped(x):
    return lax.ppermute(x, "tp", [(0, 1), (1, 0)])


def crossed(x, flip):
    places = [(pair, core) for pair in range(2) for core in range(2)]
    moves = [(2 * p + c, 2 * (1 - p) + (1 - c if flip else c)) for p, c in places]
    return lax.ppermute(x, (PAIR, "tp"), moves)


def gathered(x, axes=KV):
    chips = lax.axis_size(axes)
    return lax.all_to_all(jnp.broadcast_to(x[None], (chips, *x.shape)), axes, 0, 0, tiled=True)


def contracted(left, right, dims):
    return lax.dot_general(
        left, right, ((dims[:1], dims[1:]), ((), ())), preferred_element_type=jnp.float32
    )


def square_sums(x):
    values = x.astype(jnp.float32)
    return jnp.sum(values * values, axis=0, keepdims=True)


CHUNK = 256


def selection(core, share):
    source = lax.broadcasted_iota(jnp.int32, (CHUNK, CHUNK // 2), 0)
    target = lax.broadcasted_iota(jnp.int32, (CHUNK, CHUNK // 2), 1)
    wanted = (target // share) * (2 * share) + core * share + target % share
    return jnp.where(source == wanted, 1.0, 0.0).astype(jnp.bfloat16)


def split_kernel(
    share,
    core_ref,
    query_ref,
    forget_ref,
    input_ref,
    gate_ref,
    out_ref,
    up_ref,
    down_ref,
    mix_gain_ref,
    ffn_gain_ref,
    mix_ref,
    own_ref,
    own_out_ref,
    near_ref,
    cross_ref,
    other_ref,
):
    core, pair = core_ref[0], core_ref[1]
    half = CHUNK // 2
    columns = query_ref.shape[0]
    hidden = down_ref.shape[0]
    span = out_ref.shape[1] // 2
    lines = out_ref.shape[0] // 2
    first = 4 * columns
    chunks = up_ref.shape[0] // CHUNK
    for own, index in ((True, core), (False, 1 - core)):
        chosen = selection(index, share)
        for chunk in range(chunks):
            source = pl.ds(chunk * CHUNK, CHUNK)
            parts = [
                part[:, source].astype(jnp.float32) * mix_gain_ref[:, source]
                for part in (query_ref, forget_ref, input_ref, gate_ref)
            ]
            rows = jnp.concatenate([part.astype(jnp.bfloat16) for part in parts], axis=0)
            picked = jnp.dot(rows, chosen, preferred_element_type=jnp.float32)
            target = mix_ref if own else other_ref
            target[:first, pl.ds(chunk * half, half)] = picked.astype(jnp.bfloat16)
        for side, ref in ((pair, own_ref if own else other_ref), (1 - pair, near_ref if own else cross_ref)):
            offset = 0 if own or ref is cross_ref else first
            for chunk in range(chunks // 2):
                place = 4 * (chunk // 2) + 2 * side + chunk % 2
                source = pl.ds(pl.multiple_of(place * CHUNK, CHUNK), CHUNK)
                raised = up_ref[source, :].astype(jnp.float32).T * ffn_gain_ref[:, source]
                rows = jnp.concatenate(
                    [raised.astype(jnp.bfloat16), down_ref[:, source]], axis=0
                )
                picked = jnp.dot(rows, chosen, preferred_element_type=jnp.float32)
                picked = picked.astype(jnp.bfloat16)
                for part in range(2):
                    lanes = pl.ds(part * chunks // 2 * half + chunk * half, half)
                    ref[offset : offset + hidden, lanes] = picked[part * hidden : (part + 1) * hidden]
        start = pl.multiple_of(index * span, span)
        if own:
            own_out_ref[...] = out_ref[:, pl.ds(start, span)]
        else:
            for piece in range(2):
                other_ref[first + hidden :, pl.ds(piece * span, span)] = out_ref[
                    pl.ds(piece * lines, lines), pl.ds(start, span)
                ]


def split_weights(share, *operands):
    columns, hidden = operands[0].shape[0], operands[6].shape[0]
    lines, width = operands[4].shape[0], operands[0].shape[1] // 2
    core = jnp.stack([lax.axis_index("tp"), lax.axis_index(PAIR)]).astype(jnp.int32)
    memory = pl.BlockSpec(memory_space=pltpu.VMEM)
    shapes = (
        (4 * columns, width),
        (hidden, width),
        (lines, operands[4].shape[1] // 2),
        (hidden, width),
        (hidden, width),
        (4 * columns + hidden + lines // 2, width),
    )
    return pl.pallas_call(
        lambda *refs: split_kernel(share, *refs),
        out_shape=[jax.ShapeDtypeStruct(shape, jnp.bfloat16) for shape in shapes],
        in_specs=[pl.BlockSpec(memory_space=pltpu.SMEM)] + [memory] * len(operands),
        out_specs=[memory] * len(shapes),
    )(core, *operands)


def per_device(
    tokens,
    w_query,
    w_forget,
    w_input,
    w_output_gate,
    gate_floor,
    head_gain,
    w_out,
    mix_gain,
    ffn_gain,
    w_up,
    w_down,
    state,
):
    chips = lax.axis_size(KV)
    cores = lax.axis_size("tp")
    rows, share = tokens.shape
    width = chips * cores * share
    seq_local, heads_local, head_size, _ = state.shape
    tokens_t = tokens.T
    columns = w_query.shape[2]
    hidden_local = w_up.shape[1]

    tp = lax.axis_index("tp")

    token_half = gathered(tokens_t).reshape(chips * share, rows)
    own_mix, own_mixer, own_out, near, cross, other = split_weights(
        share,
        *[w[:, 0, :].T for w in (w_query, w_forget, w_input, w_output_gate)],
        w_out.T,
        w_up,
        w_down,
        mix_gain[None, :],
        ffn_gain[None, :],
    )
    lent = swapped(other)
    first = 4 * columns
    second = first + hidden_local
    span = lent.shape[1] // 2
    lent_out = jnp.concatenate([lent[second:, :span], lent[second:, span:]], axis=0)
    mixer_pair = jnp.concatenate([own_mixer, lent[first:second]], axis=0)
    lent_mix, own_mix, own_out, lent_out, mixer_pair = lax.optimization_barrier(
        (lent[:first], own_mix, own_out, lent_out, mixer_pair)
    )
    sums = square_sums(token_half)
    high = sums.astype(jnp.bfloat16).astype(jnp.float32)
    place = lax.broadcasted_iota(jnp.int32, (128 - 4 * columns, rows), 0)
    extra = jnp.where(place == 0, high, jnp.where(place == 1, sums - high, 0.0))
    own = contracted(own_mix, token_half, (1, 0))
    theirs = contracted(lent_mix, token_half, (1, 0))
    first, second = jnp.where(tp == 0, own, theirs), jnp.where(tp == 0, theirs, own)
    raw = jnp.stack(
        [jnp.concatenate([part, extra], axis=0).T for part in (first, second)]
    ).astype(jnp.bfloat16)
    raw = raw.reshape(cores * chips, seq_local, 128)
    raw, near, cross = lax.optimization_barrier((raw, near, cross))
    near = crossed(near, False)
    raw = lax.all_to_all(raw, ("tp", *KV), split_axis=0, concat_axis=0, tiled=True)
    raw, gate_floor, head_gain = lax.optimization_barrier((raw, gate_floor, head_gain))
    raw = raw.reshape(cores, chips, seq_local, 128).astype(jnp.float32).sum(axis=0)
    sums = raw[0, :, 4 * columns : 4 * columns + 2].sum(axis=1)
    scale = lax.rsqrt(sums / width + EPSILON)
    raw = raw[:, :, : 4 * columns] * scale[None, :, None]
    raw = raw.reshape(chips, seq_local, 4, columns).transpose(2, 1, 0, 3)
    raw = raw.reshape(4, seq_local, heads_local, head_size)
    query_vec = raw[0] * head_size ** (-0.5)
    floor_heads = gate_floor.reshape(heads_local, head_size)
    forget_gate = floor_heads + (1.0 - floor_heads) * jax.nn.sigmoid(raw[1])
    input_vec = raw[2]
    gate_vec = raw[3]
    new_state = (
        forget_gate[..., None] * state + (1.0 - forget_gate)[..., None] * input_vec[:, :, None, :]
    )
    new_state = lax.optimization_barrier(new_state)
    head_out = jnp.sum(query_vec[..., None] * new_state, axis=2)
    branch = rms_scale(head_out, head_gain) * jax.nn.silu(gate_vec)
    branch = branch.reshape(seq_local, heads_local * head_size).astype(jnp.bfloat16)

    branch, near, cross = lax.optimization_barrier((branch, near, cross))
    cross = crossed(cross, True)

    branch_half = gathered(branch).reshape(rows, heads_local * head_size)
    theirs = swapped(contracted(lent_out, branch_half, (1, 1)))
    projected = contracted(own_out, branch_half, (1, 1)) + theirs
    residual = (tokens_t.astype(jnp.float32) + projected).astype(jnp.bfloat16)

    mixer = jnp.concatenate([mixer_pair, near, cross], axis=0)
    quarter = mixer.shape[1] // 2
    up, down = mixer[:, :quarter], mixer[:, quarter:]
    residual, up, down = lax.optimization_barrier((residual, up, down))
    residual_quarter = gathered(residual, SIDE).reshape(quarter, rows)
    partial = contracted(up, residual_quarter, (1, 0))
    sums = square_sums(residual_quarter)
    units = partial.shape[0]
    arrived = swapped(jnp.concatenate([partial, sums], axis=0))
    blocks = [arrived[n * hidden_local : (n + 1) * hidden_local] for n in (1, 0, 3, 2)]
    paired = partial + jnp.concatenate(blocks, axis=0)
    sums = sums + arrived[units:]
    high = sums.astype(jnp.bfloat16).astype(jnp.float32)
    arrived = crossed(
        jnp.concatenate([paired, high, sums - high], axis=0).astype(jnp.bfloat16), False
    ).astype(jnp.float32)
    upward = paired + jnp.concatenate([arrived[units // 2 : units], arrived[: units // 2]], axis=0)
    sums = sums + arrived[units : units + 1] + arrived[units + 1 :]
    scale = lax.rsqrt(sums / width + EPSILON)
    hidden = jnp.square(jax.nn.relu(upward * scale)).astype(jnp.bfloat16)

    terms = contracted(down, hidden, (0, 0)).astype(jnp.bfloat16)
    terms = lax.all_to_all(
        terms.reshape(-1, share, rows), SIDE, split_axis=0, concat_axis=0, tiled=True
    )
    summed = terms.astype(jnp.float32).sum(axis=0)
    mixed = (residual.astype(jnp.float32) + summed).astype(jnp.bfloat16).T
    return (mixed, new_state)


def solution(mesh):
    torus = Mesh(
        mesh.devices.reshape(mesh.shape["dp"], 4, 2, 8, mesh.shape["tp"]), ("dp", *KV_TP)
    )
    placed = (
        P("dp", KV_TP),
        P(None, "tp", KV),
        P(None, "tp", KV),
        P(None, "tp", KV),
        P(None, "tp", KV),
        P("tp"),
        P(),
        P(None, KV_TP),
        P(),
        P(),
        P(None, KV_TP),
        P(KV_TP, None),
        P(DP_KV, "tp", None, None),
    )

    return jax.shard_map(
        per_device,
        mesh=torus,
        in_specs=placed,
        out_specs=(P("dp", KV_TP), P(DP_KV, "tp", None, None)),
        check_vma=False,
    )
```

```python
import jax
import jax.numpy as jnp
from jax import lax
from jax.experimental import pallas as pl
from jax.experimental.pallas import tpu as pltpu
from jax.sharding import Mesh
from jax.sharding import PartitionSpec as P


KV = ("za", "zb", "zc", "ya", "yb", "yc")
SPREAD = ("zc", "yc", "zb", "yb", "ya", "za")
KV_TP = (*KV, "tp")
DP_KV = ("dp", *KV)


EPSILON = 1e-06


def rms_scale(values, gain):
    return values * lax.rsqrt(jnp.mean(values * values, axis=-1, keepdims=True) + EPSILON) * gain


def swapped(x):
    return lax.ppermute(x, "tp", [(0, 1), (1, 0)])


def gathered(x, axes=KV):
    chips = lax.axis_size(axes)
    return lax.all_to_all(jnp.broadcast_to(x[None], (chips, *x.shape)), axes, 0, 0, tiled=True)


def contracted(left, right, dims):
    return lax.dot_general(
        left, right, ((dims[:1], dims[1:]), ((), ())), preferred_element_type=jnp.float32
    )


def square_sums(x):
    values = x.astype(jnp.float32)
    return jnp.sum(values * values, axis=0, keepdims=True)


TILE = 128


def selection(core, share):
    source = lax.broadcasted_iota(jnp.int32, (4 * TILE, 2 * TILE), 0)
    target = lax.broadcasted_iota(jnp.int32, (4 * TILE, 2 * TILE), 1)
    row, place = target // TILE, target % TILE
    wanted = (place // share) * TILE + row * 2 * share + core * share + place % share
    return jnp.where(source == wanted, 1.0, 0.0).astype(jnp.bfloat16)


def spread_tiles():
    for zc in range(2):
        for zb in range(2):
            for yb in range(2):
                chips = [
                    32 * za + 16 * zb + 8 * zc + 4 * ya + 2 * yb for ya in range(2) for za in range(2)
                ]
                yield [chip // 2 for chip in chips], [8 * zc + 4 * yc + 2 * zb + yb for yc in range(2)]


def split_kernel(
    share,
    core_ref,
    query_ref,
    forget_ref,
    input_ref,
    gate_ref,
    out_ref,
    up_ref,
    down_ref,
    mix_gain_ref,
    ffn_gain_ref,
    mix_ref,
    own_up_ref,
    own_down_ref,
    own_out_ref,
    other_ref,
):
    core = core_ref[0]
    columns = query_ref.shape[0]
    hidden = down_ref.shape[0]
    span = out_ref.shape[1] // 2
    lines = out_ref.shape[0] // 2
    first, second = 4 * columns, 4 * columns + hidden
    for tiles, places in spread_tiles():
        spans = [pl.ds(tile * TILE, TILE) for tile in tiles]
        mix_gain = jnp.concatenate([mix_gain_ref[:, part] for part in spans], axis=1)
        ffn_gain = jnp.concatenate([ffn_gain_ref[:, part] for part in spans], axis=1)
        parts = [
            jnp.concatenate([ref[:, part] for part in spans], axis=1).astype(jnp.float32) * mix_gain
            for ref in (query_ref, forget_ref, input_ref, gate_ref)
        ]
        raised = jnp.concatenate([up_ref[part, :] for part in spans], axis=0)
        parts.append(raised.astype(jnp.float32).T * ffn_gain)
        rows = [part.astype(jnp.bfloat16) for part in parts]
        rows.append(jnp.concatenate([down_ref[:, part] for part in spans], axis=1))
        rows = jnp.concatenate(rows, axis=0)
        for own, index in ((True, core), (False, 1 - core)):
            picked = jnp.dot(rows, selection(index, share), preferred_element_type=jnp.float32)
            picked = picked.astype(jnp.bfloat16)
            for row, place in enumerate(places):
                block = picked[:, row * TILE : (row + 1) * TILE]
                target = pl.ds(place * TILE, TILE)
                if own:
                    mix_ref[:, target] = block[:first]
                    own_up_ref[:, target] = block[first:second]
                    own_down_ref[:, target] = block[second:]
                else:
                    other_ref[: second + hidden, target] = block
    for own, index in ((True, core), (False, 1 - core)):
        start = pl.multiple_of(index * span, span)
        if own:
            own_out_ref[...] = out_ref[:, pl.ds(start, span)]
        else:
            for piece in range(2):
                other_ref[second + hidden :, pl.ds(piece * span, span)] = out_ref[
                    pl.ds(piece * lines, lines), pl.ds(start, span)
                ]


def split_weights(share, *operands):
    columns, hidden = operands[0].shape[0], operands[6].shape[0]
    lines, width = operands[4].shape[0], operands[0].shape[1] // 2
    core = lax.axis_index("tp").astype(jnp.int32).reshape(1)
    memory = pl.BlockSpec(memory_space=pltpu.VMEM)
    shapes = (
        (4 * columns, width),
        (hidden, width),
        (hidden, width),
        (lines, operands[4].shape[1] // 2),
        (4 * columns + 2 * hidden + lines // 2, width),
    )
    return pl.pallas_call(
        lambda *refs: split_kernel(share, *refs),
        out_shape=[jax.ShapeDtypeStruct(shape, jnp.bfloat16) for shape in shapes],
        in_specs=[pl.BlockSpec(memory_space=pltpu.SMEM)] + [memory] * len(operands),
        out_specs=[memory] * len(shapes),
    )(core, *operands)


def per_device(
    tokens,
    w_query,
    w_forget,
    w_input,
    w_output_gate,
    gate_floor,
    head_gain,
    w_out,
    mix_gain,
    ffn_gain,
    w_up,
    w_down,
    state,
):
    chips = lax.axis_size(KV)
    cores = lax.axis_size("tp")
    rows, share = tokens.shape
    width = chips * cores * share
    seq_local, heads_local, head_size, _ = state.shape
    tokens_t = tokens.T
    columns = w_query.shape[2]
    hidden_local = w_up.shape[1]

    tp = lax.axis_index("tp")

    token_half = gathered(tokens_t, SPREAD).reshape(chips * share, rows)
    own_mix, own_up, own_down, own_out, other = split_weights(
        share,
        *[w[:, 0, :].T for w in (w_query, w_forget, w_input, w_output_gate)],
        w_out.T,
        w_up,
        w_down,
        mix_gain[None, :],
        ffn_gain[None, :],
    )
    lent = swapped(other)
    first = 4 * columns
    second, third = first + hidden_local, first + 2 * hidden_local
    span = lent.shape[1] // 2
    lent_out = jnp.concatenate([lent[third:, :span], lent[third:, span:]], axis=0)
    up_both = jnp.concatenate([own_up, lent[first:second]], axis=0)
    down_both = jnp.concatenate([own_down, lent[second:third]], axis=0)
    lent_mix, own_mix, own_out, lent_out, up_both, down_both = lax.optimization_barrier(
        (lent[:first], own_mix, own_out, lent_out, up_both, down_both)
    )
    sums = square_sums(token_half)
    high = sums.astype(jnp.bfloat16).astype(jnp.float32)
    place = lax.broadcasted_iota(jnp.int32, (128 - 4 * columns, rows), 0)
    extra = jnp.where(place == 0, high, jnp.where(place == 1, sums - high, 0.0))
    own = contracted(own_mix, token_half, (1, 0))
    theirs = contracted(lent_mix, token_half, (1, 0))
    first, second = jnp.where(tp == 0, own, theirs), jnp.where(tp == 0, theirs, own)
    raw = jnp.stack(
        [jnp.concatenate([part, extra], axis=0).T for part in (first, second)]
    ).astype(jnp.bfloat16)
    raw = raw.reshape(cores * chips, seq_local, 128)
    raw = lax.all_to_all(raw, ("tp", *KV), split_axis=0, concat_axis=0, tiled=True)
    raw, gate_floor, head_gain = lax.optimization_barrier((raw, gate_floor, head_gain))
    raw = raw.reshape(cores, chips, seq_local, 128).astype(jnp.float32).sum(axis=0)
    sums = raw[0, :, 4 * columns : 4 * columns + 2].sum(axis=1)
    scale = lax.rsqrt(sums / width + EPSILON)
    raw = raw[:, :, : 4 * columns] * scale[None, :, None]
    raw = raw.reshape(chips, seq_local, 4, columns).transpose(2, 1, 0, 3)
    raw = raw.reshape(4, seq_local, heads_local, head_size)
    query_vec = raw[0] * head_size ** (-0.5)
    floor_heads = gate_floor.reshape(heads_local, head_size)
    forget_gate = floor_heads + (1.0 - floor_heads) * jax.nn.sigmoid(raw[1])
    input_vec = raw[2]
    gate_vec = raw[3]
    new_state = (
        forget_gate[..., None] * state + (1.0 - forget_gate)[..., None] * input_vec[:, :, None, :]
    )
    new_state = lax.optimization_barrier(new_state)
    head_out = jnp.sum(query_vec[..., None] * new_state, axis=2)
    branch = rms_scale(head_out, head_gain) * jax.nn.silu(gate_vec)
    branch = branch.reshape(seq_local, heads_local * head_size).astype(jnp.bfloat16)

    branch_half = gathered(branch).reshape(rows, heads_local * head_size)
    theirs = swapped(contracted(lent_out, branch_half, (1, 1)))
    projected = contracted(own_out, branch_half, (1, 1)) + theirs
    residual = (tokens_t.astype(jnp.float32) + projected).astype(jnp.bfloat16)

    residual_half = gathered(residual, SPREAD).reshape(chips * share, rows)
    partial = contracted(up_both, residual_half, (1, 0))
    sums = square_sums(residual_half)
    arrived = swapped(jnp.concatenate([partial, sums], axis=0))
    upward = partial + jnp.concatenate(
        [arrived[hidden_local : 2 * hidden_local], arrived[:hidden_local]], axis=0
    )
    scale = lax.rsqrt((sums + arrived[-1:]) / width + EPSILON)
    hidden = jnp.square(jax.nn.relu(upward * scale)).astype(jnp.bfloat16)

    terms = contracted(down_both, hidden, (0, 0)).astype(jnp.bfloat16)
    terms = lax.all_to_all(
        terms.reshape(chips, share, rows), SPREAD, split_axis=0, concat_axis=0, tiled=True
    )
    summed = terms.astype(jnp.float32).sum(axis=0)
    mixed = (residual.astype(jnp.float32) + summed).astype(jnp.bfloat16).T
    return (mixed, new_state)


def solution(mesh):
    torus = Mesh(
        mesh.devices.reshape(mesh.shape["dp"], *[2] * 6, mesh.shape["tp"]), ("dp", *KV_TP)
    )
    placed = (
        P("dp", KV_TP),
        P(None, "tp", KV),
        P(None, "tp", KV),
        P(None, "tp", KV),
        P(None, "tp", KV),
        P("tp"),
        P(),
        P(None, KV_TP),
        P(),
        P(),
        P(None, KV_TP),
        P(KV_TP, None),
        P(DP_KV, "tp", None, None),
    )

    return jax.shard_map(
        per_device,
        mesh=torus,
        in_specs=placed,
        out_specs=(P("dp", KV_TP), P(DP_KV, "tp", None, None)),
        check_vma=False,
    )
```

```python
import jax
import jax.numpy as jnp
from jax import lax
from jax.experimental import pallas as pl
from jax.experimental.pallas import tpu as pltpu
from jax.sharding import Mesh
from jax.sharding import PartitionSpec as P


KV = ("kv_0", "kv_1")
KV_TP = ("kv_0", "kv_1", "tp")
DP_KV = ("dp", "kv_0", "kv_1")


EPSILON = 1e-06


def rms_scale(values, gain):
    return values * lax.rsqrt(jnp.mean(values * values, axis=-1, keepdims=True) + EPSILON) * gain


def swapped(x):
    return lax.ppermute(x, "tp", [(0, 1), (1, 0)])


def gathered(x):
    chips = lax.axis_size(KV)
    return lax.all_to_all(jnp.broadcast_to(x[None], (chips, *x.shape)), KV, 0, 0, tiled=True)


def contracted(left, right, dims):
    return lax.dot_general(
        left, right, ((dims[:1], dims[1:]), ((), ())), preferred_element_type=jnp.float32
    )


def square_sums(x):
    values = x.astype(jnp.float32)
    return jnp.sum(values * values, axis=0, keepdims=True)


CHUNK = 256


def selection(core, share):
    source = lax.broadcasted_iota(jnp.int32, (CHUNK, CHUNK // 2), 0)
    target = lax.broadcasted_iota(jnp.int32, (CHUNK, CHUNK // 2), 1)
    wanted = (target // share) * (2 * share) + core * share + target % share
    return jnp.where(source == wanted, 1.0, 0.0).astype(jnp.bfloat16)


def split_kernel(
    share,
    core_ref,
    query_ref,
    forget_ref,
    input_ref,
    gate_ref,
    out_ref,
    up_ref,
    down_ref,
    mix_gain_ref,
    ffn_gain_ref,
    mix_ref,
    own_up_ref,
    own_down_ref,
    own_out_ref,
    other_ref,
):
    core = core_ref[0]
    half = CHUNK // 2
    columns = query_ref.shape[0]
    hidden = down_ref.shape[0]
    span = out_ref.shape[1] // 2
    lines = out_ref.shape[0] // 2
    first, second = 4 * columns, 4 * columns + hidden
    for own, index in ((True, core), (False, 1 - core)):
        chosen = selection(index, share)
        for chunk in range(up_ref.shape[0] // CHUNK):
            source = pl.ds(chunk * CHUNK, CHUNK)
            target = pl.ds(chunk * half, half)
            parts = [
                part[:, source].astype(jnp.float32) * mix_gain_ref[:, source]
                for part in (query_ref, forget_ref, input_ref, gate_ref)
            ]
            parts.append(up_ref[source, :].astype(jnp.float32).T * ffn_gain_ref[:, source])
            rows = jnp.concatenate([part.astype(jnp.bfloat16) for part in parts], axis=0)
            rows = jnp.concatenate([rows, down_ref[:, source]], axis=0)
            picked = jnp.dot(rows, chosen, preferred_element_type=jnp.float32)
            picked = picked.astype(jnp.bfloat16)
            if own:
                mix_ref[:, target] = picked[:first]
                own_up_ref[:, target] = picked[first:second]
                own_down_ref[:, target] = picked[second:]
            else:
                other_ref[: second + hidden, target] = picked
        start = pl.multiple_of(index * span, span)
        if own:
            own_out_ref[...] = out_ref[:, pl.ds(start, span)]
        else:
            for piece in range(2):
                other_ref[second + hidden :, pl.ds(piece * span, span)] = out_ref[
                    pl.ds(piece * lines, lines), pl.ds(start, span)
                ]


def split_weights(share, *operands):
    columns, hidden = operands[0].shape[0], operands[6].shape[0]
    lines, width = operands[4].shape[0], operands[0].shape[1] // 2
    core = lax.axis_index("tp").astype(jnp.int32).reshape(1)
    memory = pl.BlockSpec(memory_space=pltpu.VMEM)
    shapes = (
        (4 * columns, width),
        (hidden, width),
        (hidden, width),
        (lines, operands[4].shape[1] // 2),
        (4 * columns + 2 * hidden + lines // 2, width),
    )
    return pl.pallas_call(
        lambda *refs: split_kernel(share, *refs),
        out_shape=[jax.ShapeDtypeStruct(shape, jnp.bfloat16) for shape in shapes],
        in_specs=[pl.BlockSpec(memory_space=pltpu.SMEM)] + [memory] * len(operands),
        out_specs=[memory] * len(shapes),
    )(core, *operands)


def per_device(
    tokens,
    w_query,
    w_forget,
    w_input,
    w_output_gate,
    gate_floor,
    head_gain,
    w_out,
    mix_gain,
    ffn_gain,
    w_up,
    w_down,
    state,
):
    chips = lax.axis_size(KV)
    cores = lax.axis_size("tp")
    rows, share = tokens.shape
    width = chips * cores * share
    seq_local, heads_local, head_size, _ = state.shape
    tokens_t = tokens.T
    columns = w_query.shape[2]
    hidden_local = w_up.shape[1]

    tp = lax.axis_index("tp")

    token_half = gathered(tokens_t).reshape(chips * share, rows)
    own_mix, own_up, own_down, own_out, other = split_weights(
        share,
        *[w[:, 0, :].T for w in (w_query, w_forget, w_input, w_output_gate)],
        w_out.T,
        w_up,
        w_down,
        mix_gain[None, :],
        ffn_gain[None, :],
    )
    lent = swapped(other)
    first = 4 * columns
    second, third = first + hidden_local, first + 2 * hidden_local
    span = lent.shape[1] // 2
    lent_out = jnp.concatenate([lent[third:, :span], lent[third:, span:]], axis=0)
    mix_both = jnp.concatenate([own_mix, lent[:first]], axis=0)
    up_both = jnp.concatenate([own_up, lent[first:second]], axis=0)
    down_both = jnp.concatenate([own_down, lent[second:third]], axis=0)
    mix_both, own_out, lent_out, up_both, down_both = lax.optimization_barrier(
        (mix_both, own_out, lent_out, up_both, down_both)
    )
    sums = square_sums(token_half)
    high = sums.astype(jnp.bfloat16).astype(jnp.float32)
    place = lax.broadcasted_iota(jnp.int32, (128 - 4 * columns, rows), 0)
    extra = jnp.where(place == 0, high, jnp.where(place == 1, sums - high, 0.0))
    products = contracted(mix_both, token_half, (1, 0))
    own, theirs = products[: 4 * columns], products[4 * columns :]
    first, second = jnp.where(tp == 0, own, theirs), jnp.where(tp == 0, theirs, own)
    raw = jnp.stack(
        [jnp.concatenate([part, extra], axis=0).T for part in (first, second)]
    ).astype(jnp.bfloat16)
    raw = raw.reshape(cores * chips, seq_local, 128)
    raw = lax.all_to_all(raw, ("tp", *KV), split_axis=0, concat_axis=0, tiled=True)
    raw, gate_floor, head_gain = lax.optimization_barrier((raw, gate_floor, head_gain))
    raw = raw.reshape(cores, chips, seq_local, 128).astype(jnp.float32).sum(axis=0)
    sums = raw[0, :, 4 * columns : 4 * columns + 2].sum(axis=1)
    scale = lax.rsqrt(sums / width + EPSILON)
    raw = raw[:, :, : 4 * columns] * scale[None, :, None]
    raw = raw.reshape(chips, seq_local, 4, columns).transpose(2, 1, 0, 3)
    raw = raw.reshape(4, seq_local, heads_local, head_size)
    raw = lax.optimization_barrier([raw[part] for part in range(4)])
    query_vec = raw[0] * head_size ** (-0.5)
    floor_heads = gate_floor.reshape(heads_local, head_size)
    forget_gate = floor_heads + (1.0 - floor_heads) * jax.nn.sigmoid(raw[1])
    input_vec = raw[2]
    gate_vec = raw[3]
    kept = jnp.sum((query_vec * forget_gate)[..., None] * state, axis=2)
    added = jnp.sum(query_vec * (1.0 - forget_gate), axis=-1, keepdims=True) * input_vec
    head_out = lax.optimization_barrier(kept) + added
    branch = rms_scale(head_out, head_gain) * jax.nn.silu(gate_vec)
    branch = branch.reshape(seq_local, heads_local * head_size).astype(jnp.bfloat16)

    branch, state, forget_gate, input_vec = lax.optimization_barrier(
        (branch, state, forget_gate, input_vec)
    )
    new_state = (
        forget_gate[..., None] * state
        + (1.0 - forget_gate)[..., None] * input_vec[:, :, None, :]
    )

    branch_half = gathered(branch).reshape(rows, heads_local * head_size)
    theirs = swapped(contracted(lent_out, branch_half, (1, 1)))
    projected = contracted(own_out, branch_half, (1, 1)) + theirs
    residual = (tokens_t.astype(jnp.float32) + projected).astype(jnp.bfloat16)

    residual_half = gathered(residual).reshape(chips * share, rows)
    partial = contracted(up_both, residual_half, (1, 0))
    sums = square_sums(residual_half)
    arrived = swapped(jnp.concatenate([partial, sums], axis=0))
    upward = partial + jnp.concatenate(
        [arrived[hidden_local : 2 * hidden_local], arrived[:hidden_local]], axis=0
    )
    scale = lax.rsqrt((sums + arrived[-1:]) / width + EPSILON)
    hidden = jnp.square(jax.nn.relu(upward * scale)).astype(jnp.bfloat16)

    terms = contracted(down_both, hidden, (0, 0)).astype(jnp.bfloat16)
    terms = lax.all_to_all(
        terms.reshape(chips, share, rows), KV, split_axis=0, concat_axis=0, tiled=True
    )
    summed = terms.astype(jnp.float32).sum(axis=0)
    mixed = (residual.astype(jnp.float32) + summed).astype(jnp.bfloat16).T
    return (mixed, new_state)


def solution(mesh):
    torus = Mesh(
        mesh.devices.reshape(mesh.shape["dp"], 8, 8, mesh.shape["tp"]), ("dp", "kv_0", "kv_1", "tp")
    )
    placed = (
        P("dp", KV_TP),
        P(None, "tp", KV),
        P(None, "tp", KV),
        P(None, "tp", KV),
        P(None, "tp", KV),
        P("tp"),
        P(),
        P(None, KV_TP),
        P(),
        P(),
        P(None, KV_TP),
        P(KV_TP, None),
        P(DP_KV, "tp", None, None),
    )

    return jax.shard_map(
        per_device,
        mesh=torus,
        in_specs=placed,
        out_specs=(P("dp", KV_TP), P(DP_KV, "tp", None, None)),
        check_vma=False,
    )
```

```python
import jax
import jax.numpy as jnp
from jax import lax
from jax.experimental import pallas as pl
from jax.experimental.pallas import tpu as pltpu
from jax.sharding import Mesh
from jax.sharding import PartitionSpec as P


KV = ("kv_0", "kv_1")
KV_TP = ("kv_0", "kv_1", "tp")
DP_KV = ("dp", "kv_0", "kv_1")


EPSILON = 1e-06


def rms_scale(values, gain):
    return values * lax.rsqrt(jnp.mean(values * values, axis=-1, keepdims=True) + EPSILON) * gain


def swapped(x):
    return lax.ppermute(x, "tp", [(0, 1), (1, 0)])


def gathered(x):
    chips = lax.axis_size(KV)
    return lax.all_to_all(jnp.broadcast_to(x[None], (chips, *x.shape)), KV, 0, 0, tiled=True)


def contracted(left, right, dims):
    return lax.dot_general(
        left, right, ((dims[:1], dims[1:]), ((), ())), preferred_element_type=jnp.float32
    )


def square_sums(x):
    values = x.astype(jnp.float32)
    return jnp.sum(values * values, axis=0, keepdims=True)


CHUNK = 256


def selection(core, share):
    source = lax.broadcasted_iota(jnp.int32, (CHUNK, CHUNK // 2), 0)
    target = lax.broadcasted_iota(jnp.int32, (CHUNK, CHUNK // 2), 1)
    wanted = (target // share) * (2 * share) + core * share + target % share
    return jnp.where(source == wanted, 1.0, 0.0).astype(jnp.bfloat16)


def split_kernel(
    share,
    core_ref,
    query_ref,
    forget_ref,
    input_ref,
    gate_ref,
    out_ref,
    up_ref,
    down_ref,
    mix_gain_ref,
    ffn_gain_ref,
    mix_ref,
    own_up_ref,
    own_down_ref,
    own_out_ref,
    other_ref,
):
    core = core_ref[0]
    half = CHUNK // 2
    columns = query_ref.shape[0]
    hidden = down_ref.shape[0]
    span = out_ref.shape[1] // 2
    lines = out_ref.shape[0] // 2
    first, second = 4 * columns, 4 * columns + hidden
    for own, index in ((True, core), (False, 1 - core)):
        chosen = selection(index, share)
        for chunk in range(up_ref.shape[0] // CHUNK):
            source = pl.ds(chunk * CHUNK, CHUNK)
            target = pl.ds(chunk * half, half)
            parts = [
                part[:, source].astype(jnp.float32) * mix_gain_ref[:, source]
                for part in (query_ref, forget_ref, input_ref, gate_ref)
            ]
            parts.append(up_ref[source, :].astype(jnp.float32).T * ffn_gain_ref[:, source])
            rows = jnp.concatenate([part.astype(jnp.bfloat16) for part in parts], axis=0)
            rows = jnp.concatenate([rows, down_ref[:, source]], axis=0)
            picked = jnp.dot(rows, chosen, preferred_element_type=jnp.float32)
            picked = picked.astype(jnp.bfloat16)
            if own:
                mix_ref[:, target] = picked[:first]
                own_up_ref[:, target] = picked[first:second]
                own_down_ref[:, target] = picked[second:]
            else:
                other_ref[: second + hidden, target] = picked
        start = pl.multiple_of(index * span, span)
        if own:
            own_out_ref[...] = out_ref[:, pl.ds(start, span)]
        else:
            for piece in range(2):
                other_ref[second + hidden :, pl.ds(piece * span, span)] = out_ref[
                    pl.ds(piece * lines, lines), pl.ds(start, span)
                ]


def split_weights(share, *operands):
    columns, hidden = operands[0].shape[0], operands[6].shape[0]
    lines, width = operands[4].shape[0], operands[0].shape[1] // 2
    core = lax.axis_index("tp").astype(jnp.int32).reshape(1)
    memory = pl.BlockSpec(memory_space=pltpu.VMEM)
    shapes = (
        (4 * columns, width),
        (hidden, width),
        (hidden, width),
        (lines, operands[4].shape[1] // 2),
        (4 * columns + 2 * hidden + lines // 2, width),
    )
    return pl.pallas_call(
        lambda *refs: split_kernel(share, *refs),
        out_shape=[jax.ShapeDtypeStruct(shape, jnp.bfloat16) for shape in shapes],
        in_specs=[pl.BlockSpec(memory_space=pltpu.SMEM)] + [memory] * len(operands),
        out_specs=[memory] * len(shapes),
    )(core, *operands)


def per_device(
    tokens,
    w_query,
    w_forget,
    w_input,
    w_output_gate,
    gate_floor,
    head_gain,
    w_out,
    mix_gain,
    ffn_gain,
    w_up,
    w_down,
    state,
):
    chips = lax.axis_size(KV)
    cores = lax.axis_size("tp")
    rows, share = tokens.shape
    width = chips * cores * share
    seq_local, heads_local, head_size, _ = state.shape
    tokens_t = tokens.T
    columns = w_query.shape[2]
    hidden_local = w_up.shape[1]

    tp = lax.axis_index("tp")

    token_half = gathered(tokens_t).reshape(chips * share, rows)
    own_mix, own_up, own_down, own_out, other = split_weights(
        share,
        *[w[:, 0, :].T for w in (w_query, w_forget, w_input, w_output_gate)],
        w_out.T,
        w_up,
        w_down,
        mix_gain[None, :],
        ffn_gain[None, :],
    )
    lent = swapped(other)
    first = 4 * columns
    second, third = first + hidden_local, first + 2 * hidden_local
    span = lent.shape[1] // 2
    lent_out = jnp.concatenate([lent[third:, :span], lent[third:, span:]], axis=0)
    up_both = jnp.concatenate([own_up, lent[first:second]], axis=0)
    down_both = jnp.concatenate([own_down, lent[second:third]], axis=0)
    lent_mix, own_mix, own_out, lent_out, up_both, down_both = lax.optimization_barrier(
        (lent[:first], own_mix, own_out, lent_out, up_both, down_both)
    )
    sums = square_sums(token_half)
    high = sums.astype(jnp.bfloat16).astype(jnp.float32)
    place = lax.broadcasted_iota(jnp.int32, (128 - 4 * columns, rows), 0)
    extra = jnp.where(place == 0, high, jnp.where(place == 1, sums - high, 0.0))
    own = contracted(own_mix, token_half, (1, 0))
    theirs = contracted(lent_mix, token_half, (1, 0))
    first, second = jnp.where(tp == 0, own, theirs), jnp.where(tp == 0, theirs, own)
    raw = jnp.stack(
        [jnp.concatenate([part, extra], axis=0).T for part in (first, second)]
    ).astype(jnp.bfloat16)
    raw = raw.reshape(cores * chips, seq_local, 128)
    raw = lax.all_to_all(raw, ("tp", *KV), split_axis=0, concat_axis=0, tiled=True)
    raw, gate_floor, head_gain = lax.optimization_barrier((raw, gate_floor, head_gain))
    raw = raw.reshape(cores, chips, seq_local, 128).astype(jnp.float32).sum(axis=0)
    sums = raw[0, :, 4 * columns : 4 * columns + 2].sum(axis=1)
    scale = lax.rsqrt(sums / width + EPSILON)
    raw = raw[:, :, : 4 * columns] * scale[None, :, None]
    raw = raw.reshape(chips, seq_local, 4, columns).transpose(2, 1, 0, 3)
    raw = raw.reshape(4, seq_local, heads_local, head_size)
    raw = lax.optimization_barrier([raw[part] for part in range(4)])
    query_vec = raw[0] * head_size ** (-0.5)
    floor_heads = gate_floor.reshape(heads_local, head_size)
    forget_gate = floor_heads + (1.0 - floor_heads) * jax.nn.sigmoid(raw[1])
    input_vec = raw[2]
    gate_vec = raw[3]
    kept = jnp.sum((query_vec * forget_gate)[..., None] * state, axis=2)
    added = jnp.sum(query_vec * (1.0 - forget_gate), axis=-1, keepdims=True) * input_vec
    head_out = lax.optimization_barrier(kept) + added
    branch = rms_scale(head_out, head_gain) * jax.nn.silu(gate_vec)
    branch = branch.reshape(seq_local, heads_local * head_size).astype(jnp.bfloat16)

    branch, state, forget_gate, input_vec = lax.optimization_barrier(
        (branch, state, forget_gate, input_vec)
    )
    given = input_vec[:, :, None, :]
    new_state = given + forget_gate[..., None] * (state - given)

    branch_half = gathered(branch).reshape(rows, heads_local * head_size)
    theirs = swapped(contracted(lent_out, branch_half, (1, 1)))
    projected = contracted(own_out, branch_half, (1, 1)) + theirs
    residual = (tokens_t.astype(jnp.float32) + projected).astype(jnp.bfloat16)

    residual_half = gathered(residual).reshape(chips * share, rows)
    partial = contracted(up_both, residual_half, (1, 0))
    sums = square_sums(residual_half)
    arrived = swapped(jnp.concatenate([partial, sums], axis=0))
    upward = partial + jnp.concatenate(
        [arrived[hidden_local : 2 * hidden_local], arrived[:hidden_local]], axis=0
    )
    scale = lax.rsqrt((sums + arrived[-1:]) / width + EPSILON)
    hidden = jnp.square(jax.nn.relu(upward * scale)).astype(jnp.bfloat16)

    terms = contracted(down_both, hidden, (0, 0)).astype(jnp.bfloat16)
    terms = lax.all_to_all(
        terms.reshape(chips, share, rows), KV, split_axis=0, concat_axis=0, tiled=True
    )
    summed = terms.astype(jnp.float32).sum(axis=0)
    mixed = (residual.astype(jnp.float32) + summed).astype(jnp.bfloat16).T
    return (mixed, new_state)


def solution(mesh):
    torus = Mesh(
        mesh.devices.reshape(mesh.shape["dp"], 8, 8, mesh.shape["tp"]), ("dp", "kv_0", "kv_1", "tp")
    )
    placed = (
        P("dp", KV_TP),
        P(None, "tp", KV),
        P(None, "tp", KV),
        P(None, "tp", KV),
        P(None, "tp", KV),
        P("tp"),
        P(),
        P(None, KV_TP),
        P(),
        P(),
        P(None, KV_TP),
        P(KV_TP, None),
        P(DP_KV, "tp", None, None),
    )

    return jax.shard_map(
        per_device,
        mesh=torus,
        in_specs=placed,
        out_specs=(P("dp", KV_TP), P(DP_KV, "tp", None, None)),
        check_vma=False,
    )
```

```python
import jax
import jax.numpy as jnp
from jax import lax
from jax.experimental import pallas as pl
from jax.experimental.pallas import tpu as pltpu
from jax.sharding import Mesh
from jax.sharding import PartitionSpec as P


KV = ("kv_0", "kv_1")
KV_TP = ("kv_0", "kv_1", "tp")
DP_KV = ("dp", "kv_0", "kv_1")


EPSILON = 1e-06


def rms_scale(values, gain):
    return values * lax.rsqrt(jnp.mean(values * values, axis=-1, keepdims=True) + EPSILON) * gain


def swapped(x):
    return lax.ppermute(x, "tp", [(0, 1), (1, 0)])


def gathered(x):
    chips = lax.axis_size(KV)
    return lax.all_to_all(jnp.broadcast_to(x[None], (chips, *x.shape)), KV, 0, 0, tiled=True)


def contracted(left, right, dims):
    return lax.dot_general(
        left, right, ((dims[:1], dims[1:]), ((), ())), preferred_element_type=jnp.float32
    )


def square_sums(x):
    values = x.astype(jnp.float32)
    return jnp.sum(values * values, axis=0, keepdims=True)


CHUNK = 256


def selection(core, share):
    source = lax.broadcasted_iota(jnp.int32, (CHUNK, CHUNK // 2), 0)
    target = lax.broadcasted_iota(jnp.int32, (CHUNK, CHUNK // 2), 1)
    wanted = (target // share) * (2 * share) + core * share + target % share
    return jnp.where(source == wanted, 1.0, 0.0).astype(jnp.bfloat16)


def split_kernel(
    share,
    core_ref,
    query_ref,
    forget_ref,
    input_ref,
    gate_ref,
    out_ref,
    up_ref,
    down_ref,
    mix_gain_ref,
    ffn_gain_ref,
    mix_ref,
    own_up_ref,
    own_down_ref,
    own_out_ref,
    other_ref,
):
    core = core_ref[0]
    half = CHUNK // 2
    columns = query_ref.shape[0]
    hidden = down_ref.shape[0]
    span = out_ref.shape[1] // 2
    lines = out_ref.shape[0] // 2
    first, second = 4 * columns, 4 * columns + hidden
    for own, index in ((True, core), (False, 1 - core)):
        chosen = selection(index, share)
        for chunk in range(up_ref.shape[0] // CHUNK):
            source = pl.ds(chunk * CHUNK, CHUNK)
            target = pl.ds(chunk * half, half)
            parts = [
                part[:, source].astype(jnp.float32) * mix_gain_ref[:, source]
                for part in (query_ref, forget_ref, input_ref, gate_ref)
            ]
            parts.append(up_ref[source, :].astype(jnp.float32).T * ffn_gain_ref[:, source])
            rows = jnp.concatenate([part.astype(jnp.bfloat16) for part in parts], axis=0)
            rows = jnp.concatenate([rows, down_ref[:, source]], axis=0)
            picked = jnp.dot(rows, chosen, preferred_element_type=jnp.float32)
            picked = picked.astype(jnp.bfloat16)
            if own:
                mix_ref[:, target] = picked[:first]
                own_up_ref[:, target] = picked[first:second]
                own_down_ref[:, target] = picked[second:]
            else:
                other_ref[: second + hidden, target] = picked
        start = pl.multiple_of(index * span, span)
        if own:
            own_out_ref[...] = out_ref[:, pl.ds(start, span)]
        else:
            for piece in range(2):
                other_ref[second + hidden :, pl.ds(piece * span, span)] = out_ref[
                    pl.ds(piece * lines, lines), pl.ds(start, span)
                ]


def split_weights(share, *operands):
    columns, hidden = operands[0].shape[0], operands[6].shape[0]
    lines, width = operands[4].shape[0], operands[0].shape[1] // 2
    core = lax.axis_index("tp").astype(jnp.int32).reshape(1)
    memory = pl.BlockSpec(memory_space=pltpu.VMEM)
    shapes = (
        (4 * columns, width),
        (hidden, width),
        (hidden, width),
        (lines, operands[4].shape[1] // 2),
        (4 * columns + 2 * hidden + lines // 2, width),
    )
    return pl.pallas_call(
        lambda *refs: split_kernel(share, *refs),
        out_shape=[jax.ShapeDtypeStruct(shape, jnp.bfloat16) for shape in shapes],
        in_specs=[pl.BlockSpec(memory_space=pltpu.SMEM)] + [memory] * len(operands),
        out_specs=[memory] * len(shapes),
    )(core, *operands)


def per_device(
    tokens,
    w_query,
    w_forget,
    w_input,
    w_output_gate,
    gate_floor,
    head_gain,
    w_out,
    mix_gain,
    ffn_gain,
    w_up,
    w_down,
    state,
):
    chips = lax.axis_size(KV)
    cores = lax.axis_size("tp")
    rows, share = tokens.shape
    width = chips * cores * share
    seq_local, heads_local, head_size, _ = state.shape
    tokens_t = tokens.T
    columns = w_query.shape[2]
    hidden_local = w_up.shape[1]

    tp = lax.axis_index("tp")

    token_half = gathered(tokens_t).reshape(chips * share, rows)
    own_mix, own_up, own_down, own_out, other = split_weights(
        share,
        *[w[:, 0, :].T for w in (w_query, w_forget, w_input, w_output_gate)],
        w_out.T,
        w_up,
        w_down,
        mix_gain[None, :],
        ffn_gain[None, :],
    )
    lent = swapped(other)
    first = 4 * columns
    second, third = first + hidden_local, first + 2 * hidden_local
    span = lent.shape[1] // 2
    lent_out = jnp.concatenate([lent[third:, :span], lent[third:, span:]], axis=0)
    down_both = jnp.concatenate([own_down, lent[second:third]], axis=0)
    lent_mix, lent_up, own_mix, own_up, own_out, lent_out, down_both = lax.optimization_barrier(
        (lent[:first], lent[first:second], own_mix, own_up, own_out, lent_out, down_both)
    )
    sums = square_sums(token_half)
    high = sums.astype(jnp.bfloat16).astype(jnp.float32)
    place = lax.broadcasted_iota(jnp.int32, (128 - 4 * columns, rows), 0)
    extra = jnp.where(place == 0, high, jnp.where(place == 1, sums - high, 0.0))
    own = contracted(own_mix, token_half, (1, 0))
    theirs = contracted(lent_mix, token_half, (1, 0))
    first, second = jnp.where(tp == 0, own, theirs), jnp.where(tp == 0, theirs, own)
    raw = jnp.stack(
        [jnp.concatenate([part, extra], axis=0).T for part in (first, second)]
    ).astype(jnp.bfloat16)
    raw = raw.reshape(cores * chips, seq_local, 128)
    raw = lax.all_to_all(raw, ("tp", *KV), split_axis=0, concat_axis=0, tiled=True)
    raw, gate_floor, head_gain = lax.optimization_barrier((raw, gate_floor, head_gain))
    raw = raw.reshape(cores, chips, seq_local, 128).astype(jnp.float32).sum(axis=0)
    sums = raw[0, :, 4 * columns : 4 * columns + 2].sum(axis=1)
    scale = lax.rsqrt(sums / width + EPSILON)
    raw = raw[:, :, : 4 * columns] * scale[None, :, None]
    raw = raw.reshape(chips, seq_local, 4, columns).transpose(2, 1, 0, 3)
    raw = raw.reshape(4, seq_local, heads_local, head_size)
    raw = lax.optimization_barrier([raw[part] for part in range(4)])
    query_vec = raw[0] * head_size ** (-0.5)
    floor_heads = gate_floor.reshape(heads_local, head_size)
    forget_gate = floor_heads + (1.0 - floor_heads) * jax.nn.sigmoid(raw[1])
    input_vec = raw[2]
    gate_vec = raw[3]
    kept = jnp.sum((query_vec * forget_gate)[..., None] * state, axis=2)
    added = jnp.sum(query_vec * (1.0 - forget_gate), axis=-1, keepdims=True) * input_vec
    head_out = lax.optimization_barrier(kept) + added
    branch = rms_scale(head_out, head_gain) * jax.nn.silu(gate_vec)
    branch = branch.reshape(seq_local, heads_local * head_size).astype(jnp.bfloat16)

    branch, state, forget_gate, input_vec = lax.optimization_barrier(
        (branch, state, forget_gate, input_vec)
    )
    given = input_vec[:, :, None, :]
    new_state = given + forget_gate[..., None] * (state - given)

    branch_half = gathered(branch).reshape(rows, heads_local * head_size)
    theirs = swapped(contracted(lent_out, branch_half, (1, 1)))
    projected = contracted(own_out, branch_half, (1, 1)) + theirs
    residual = (tokens_t.astype(jnp.float32) + projected).astype(jnp.bfloat16)

    residual_half = gathered(residual).reshape(chips * share, rows)
    partial = jnp.concatenate(
        [contracted(up, residual_half, (1, 0)) for up in (own_up, lent_up)], axis=0
    )
    sums = square_sums(residual_half)
    arrived = swapped(jnp.concatenate([partial, sums], axis=0))
    upward = partial + jnp.concatenate(
        [arrived[hidden_local : 2 * hidden_local], arrived[:hidden_local]], axis=0
    )
    scale = lax.rsqrt((sums + arrived[-1:]) / width + EPSILON)
    hidden = jnp.square(jax.nn.relu(upward * scale)).astype(jnp.bfloat16)

    terms = contracted(down_both, hidden, (0, 0)).astype(jnp.bfloat16)
    terms = lax.all_to_all(
        terms.reshape(chips, share, rows), KV, split_axis=0, concat_axis=0, tiled=True
    )
    summed = terms.astype(jnp.float32).sum(axis=0)
    mixed = (residual.astype(jnp.float32) + summed).astype(jnp.bfloat16).T
    return (mixed, new_state)


def solution(mesh):
    torus = Mesh(
        mesh.devices.reshape(mesh.shape["dp"], 8, 8, mesh.shape["tp"]), ("dp", "kv_0", "kv_1", "tp")
    )
    placed = (
        P("dp", KV_TP),
        P(None, "tp", KV),
        P(None, "tp", KV),
        P(None, "tp", KV),
        P(None, "tp", KV),
        P("tp"),
        P(),
        P(None, KV_TP),
        P(),
        P(),
        P(None, KV_TP),
        P(KV_TP, None),
        P(DP_KV, "tp", None, None),
    )

    return jax.shard_map(
        per_device,
        mesh=torus,
        in_specs=placed,
        out_specs=(P("dp", KV_TP), P(DP_KV, "tp", None, None)),
        check_vma=False,
    )
```

```python
import jax
import jax.numpy as jnp
from jax import lax
from jax.experimental import pallas as pl
from jax.experimental.pallas import tpu as pltpu
from jax.sharding import Mesh
from jax.sharding import PartitionSpec as P


KV = ("kv_0", "kv_1")
KV_TP = ("kv_0", "kv_1", "tp")
DP_KV = ("dp", "kv_0", "kv_1")


EPSILON = 1e-06


def rms_scale(values, gain):
    return values * lax.rsqrt(jnp.mean(values * values, axis=-1, keepdims=True) + EPSILON) * gain


def swapped(x):
    return lax.ppermute(x, "tp", [(0, 1), (1, 0)])


def gathered(x):
    chips = lax.axis_size(KV)
    return lax.all_to_all(jnp.broadcast_to(x[None], (chips, *x.shape)), KV, 0, 0, tiled=True)


def contracted(left, right, dims):
    return lax.dot_general(
        left, right, ((dims[:1], dims[1:]), ((), ())), preferred_element_type=jnp.float32
    )


def square_sums(x):
    values = x.astype(jnp.float32)
    return jnp.sum(values * values, axis=0, keepdims=True)


CHUNK = 256


def selection(core, share):
    source = lax.broadcasted_iota(jnp.int32, (CHUNK, CHUNK // 2), 0)
    target = lax.broadcasted_iota(jnp.int32, (CHUNK, CHUNK // 2), 1)
    wanted = (target // share) * (2 * share) + core * share + target % share
    return jnp.where(source == wanted, 1.0, 0.0).astype(jnp.bfloat16)


def split_kernel(
    share,
    core_ref,
    query_ref,
    forget_ref,
    input_ref,
    gate_ref,
    out_ref,
    up_ref,
    down_ref,
    mix_gain_ref,
    ffn_gain_ref,
    mix_ref,
    own_up_ref,
    own_down_ref,
    own_out_ref,
    other_ref,
    other_up_ref,
    other_down_ref,
):
    core = core_ref[0]
    half = CHUNK // 2
    columns = query_ref.shape[0]
    hidden = down_ref.shape[0]
    span = out_ref.shape[1] // 2
    lines = out_ref.shape[0] // 2
    first, second = 4 * columns, 4 * columns + hidden
    for own, index in ((True, core), (False, 1 - core)):
        chosen = selection(index, share)
        for chunk in range(up_ref.shape[0] // CHUNK):
            source = pl.ds(chunk * CHUNK, CHUNK)
            target = pl.ds(chunk * half, half)
            parts = [
                part[:, source].astype(jnp.float32) * mix_gain_ref[:, source]
                for part in (query_ref, forget_ref, input_ref, gate_ref)
            ]
            parts.append(up_ref[source, :].astype(jnp.float32).T * ffn_gain_ref[:, source])
            rows = jnp.concatenate([part.astype(jnp.bfloat16) for part in parts], axis=0)
            rows = jnp.concatenate([rows, down_ref[:, source]], axis=0)
            picked = jnp.dot(rows, chosen, preferred_element_type=jnp.float32)
            picked = picked.astype(jnp.bfloat16)
            if own:
                mix_ref[:, target] = picked[:first]
                own_up_ref[:, target] = picked[first:second]
                own_down_ref[:, target] = picked[second:]
            else:
                other_ref[:first, target] = picked[:first]
                other_up_ref[:, target] = picked[first:second]
                other_down_ref[:, target] = picked[second:]
        start = pl.multiple_of(index * span, span)
        if own:
            own_out_ref[...] = out_ref[:, pl.ds(start, span)]
        else:
            for piece in range(2):
                other_ref[first:, pl.ds(piece * span, span)] = out_ref[
                    pl.ds(piece * lines, lines), pl.ds(start, span)
                ]


def split_weights(share, *operands):
    columns, hidden = operands[0].shape[0], operands[6].shape[0]
    lines, width = operands[4].shape[0], operands[0].shape[1] // 2
    core = lax.axis_index("tp").astype(jnp.int32).reshape(1)
    memory = pl.BlockSpec(memory_space=pltpu.VMEM)
    shapes = (
        (4 * columns, width),
        (hidden, width),
        (hidden, width),
        (lines, operands[4].shape[1] // 2),
        (4 * columns + lines // 2, width),
        (hidden, width),
        (hidden, width),
    )
    return pl.pallas_call(
        lambda *refs: split_kernel(share, *refs),
        out_shape=[jax.ShapeDtypeStruct(shape, jnp.bfloat16) for shape in shapes],
        in_specs=[pl.BlockSpec(memory_space=pltpu.SMEM)] + [memory] * len(operands),
        out_specs=[memory] * len(shapes),
    )(core, *operands)


def per_device(
    tokens,
    w_query,
    w_forget,
    w_input,
    w_output_gate,
    gate_floor,
    head_gain,
    w_out,
    mix_gain,
    ffn_gain,
    w_up,
    w_down,
    state,
):
    chips = lax.axis_size(KV)
    cores = lax.axis_size("tp")
    rows, share = tokens.shape
    width = chips * cores * share
    seq_local, heads_local, head_size, _ = state.shape
    tokens_t = tokens.T
    columns = w_query.shape[2]
    hidden_local = w_up.shape[1]

    tp = lax.axis_index("tp")

    token_half = gathered(tokens_t).reshape(chips * share, rows)
    own_mix, own_up, own_down, own_out, other, other_up, other_down = split_weights(
        share,
        *[w[:, 0, :].T for w in (w_query, w_forget, w_input, w_output_gate)],
        w_out.T,
        w_up,
        w_down,
        mix_gain[None, :],
        ffn_gain[None, :],
    )
    lent = swapped(other)
    first = 4 * columns
    span = lent.shape[1] // 2
    lent_out = jnp.concatenate([lent[first:, :span], lent[first:, span:]], axis=0)
    lent_mix, own_mix, own_out, lent_out = lax.optimization_barrier(
        (lent[:first], own_mix, own_out, lent_out)
    )
    lent_up, lent_down = swapped(other_up), swapped(other_down)
    sums = square_sums(token_half)
    high = sums.astype(jnp.bfloat16).astype(jnp.float32)
    place = lax.broadcasted_iota(jnp.int32, (128 - 4 * columns, rows), 0)
    extra = jnp.where(place == 0, high, jnp.where(place == 1, sums - high, 0.0))
    own = contracted(own_mix, token_half, (1, 0))
    theirs = contracted(lent_mix, token_half, (1, 0))
    first, second = jnp.where(tp == 0, own, theirs), jnp.where(tp == 0, theirs, own)
    raw = jnp.stack(
        [jnp.concatenate([part, extra], axis=0).T for part in (first, second)]
    ).astype(jnp.bfloat16)
    raw = raw.reshape(cores * chips, seq_local, 128)
    raw = lax.all_to_all(raw, ("tp", *KV), split_axis=0, concat_axis=0, tiled=True)
    raw, gate_floor, head_gain = lax.optimization_barrier((raw, gate_floor, head_gain))
    raw = raw.reshape(cores, chips, seq_local, 128).astype(jnp.float32).sum(axis=0)
    sums = raw[0, :, 4 * columns : 4 * columns + 2].sum(axis=1)
    scale = lax.rsqrt(sums / width + EPSILON)
    raw = raw[:, :, : 4 * columns] * scale[None, :, None]
    raw = raw.reshape(chips, seq_local, 4, columns).transpose(2, 1, 0, 3)
    raw = raw.reshape(4, seq_local, heads_local, head_size)
    raw = lax.optimization_barrier([raw[part] for part in range(4)])
    query_vec = raw[0] * head_size ** (-0.5)
    floor_heads = gate_floor.reshape(heads_local, head_size)
    forget_gate = floor_heads + (1.0 - floor_heads) * jax.nn.sigmoid(raw[1])
    input_vec = raw[2]
    gate_vec = raw[3]
    kept = jnp.sum((query_vec * forget_gate)[..., None] * state, axis=2)
    added = jnp.sum(query_vec * (1.0 - forget_gate), axis=-1, keepdims=True) * input_vec
    head_out = lax.optimization_barrier(kept) + added
    branch = rms_scale(head_out, head_gain) * jax.nn.silu(gate_vec)
    branch = branch.reshape(seq_local, heads_local * head_size).astype(jnp.bfloat16)

    branch, state, forget_gate, input_vec = lax.optimization_barrier(
        (branch, state, forget_gate, input_vec)
    )
    given = input_vec[:, :, None, :]
    new_state = given + forget_gate[..., None] * (state - given)

    branch_half = gathered(branch).reshape(rows, heads_local * head_size)
    theirs = swapped(contracted(lent_out, branch_half, (1, 1)))
    projected = contracted(own_out, branch_half, (1, 1)) + theirs
    residual = (tokens_t.astype(jnp.float32) + projected).astype(jnp.bfloat16)

    residual_half = gathered(residual).reshape(chips * share, rows)
    partial = jnp.concatenate(
        [contracted(up, residual_half, (1, 0)) for up in (own_up, lent_up)], axis=0
    )
    sums = square_sums(residual_half)
    arrived = swapped(jnp.concatenate([partial, sums], axis=0))
    upward = partial + jnp.concatenate(
        [arrived[hidden_local : 2 * hidden_local], arrived[:hidden_local]], axis=0
    )
    scale = lax.rsqrt((sums + arrived[-1:]) / width + EPSILON)
    hidden = jnp.square(jax.nn.relu(upward * scale)).astype(jnp.bfloat16)

    down_both = jnp.concatenate([own_down, lent_down], axis=0)
    terms = contracted(down_both, hidden, (0, 0)).astype(jnp.bfloat16)
    terms = lax.all_to_all(
        terms.reshape(chips, share, rows), KV, split_axis=0, concat_axis=0, tiled=True
    )
    summed = terms.astype(jnp.float32).sum(axis=0)
    mixed = (residual.astype(jnp.float32) + summed).astype(jnp.bfloat16).T
    return (mixed, new_state)


def solution(mesh):
    torus = Mesh(
        mesh.devices.reshape(mesh.shape["dp"], 8, 8, mesh.shape["tp"]), ("dp", "kv_0", "kv_1", "tp")
    )
    placed = (
        P("dp", KV_TP),
        P(None, "tp", KV),
        P(None, "tp", KV),
        P(None, "tp", KV),
        P(None, "tp", KV),
        P("tp"),
        P(),
        P(None, KV_TP),
        P(),
        P(),
        P(None, KV_TP),
        P(KV_TP, None),
        P(DP_KV, "tp", None, None),
    )

    return jax.shard_map(
        per_device,
        mesh=torus,
        in_specs=placed,
        out_specs=(P("dp", KV_TP), P(DP_KV, "tp", None, None)),
        check_vma=False,
    )
```

```python
import jax
import jax.numpy as jnp
from jax import lax
from jax.experimental import pallas as pl
from jax.experimental.pallas import tpu as pltpu
from jax.sharding import Mesh
from jax.sharding import PartitionSpec as P


KV = ("kv_0", "kv_1")
KV_TP = ("kv_0", "kv_1", "tp")
DP_KV = ("dp", "kv_0", "kv_1")


EPSILON = 1e-06


def rms_scale(values, gain):
    return values * lax.rsqrt(jnp.mean(values * values, axis=-1, keepdims=True) + EPSILON) * gain


def swapped(x):
    return lax.ppermute(x, "tp", [(0, 1), (1, 0)])


def gathered(x):
    chips = lax.axis_size(KV)
    return lax.all_to_all(jnp.broadcast_to(x[None], (chips, *x.shape)), KV, 0, 0, tiled=True)


def contracted(left, right, dims):
    return lax.dot_general(
        left, right, ((dims[:1], dims[1:]), ((), ())), preferred_element_type=jnp.float32
    )


def square_sums(x):
    values = x.astype(jnp.float32)
    return jnp.sum(values * values, axis=0, keepdims=True)


CHUNK = 256


def selection(core, share):
    source = lax.broadcasted_iota(jnp.int32, (CHUNK, CHUNK // 2), 0)
    target = lax.broadcasted_iota(jnp.int32, (CHUNK, CHUNK // 2), 1)
    wanted = (target // share) * (2 * share) + core * share + target % share
    return jnp.where(source == wanted, 1.0, 0.0).astype(jnp.bfloat16)


def split_kernel(
    share,
    core_ref,
    query_ref,
    forget_ref,
    input_ref,
    gate_ref,
    out_ref,
    up_ref,
    down_ref,
    mix_gain_ref,
    ffn_gain_ref,
    mix_ref,
    own_up_ref,
    own_down_ref,
    own_out_ref,
    other_ref,
    other_up_ref,
    other_down_ref,
):
    core = core_ref[0]
    half = CHUNK // 2
    columns = query_ref.shape[0]
    hidden = down_ref.shape[0]
    span = out_ref.shape[1] // 2
    lines = out_ref.shape[0] // 2
    first, second = 4 * columns, 4 * columns + hidden
    for own, index in ((True, core), (False, 1 - core)):
        chosen = selection(index, share)
        for chunk in range(up_ref.shape[0] // CHUNK):
            source = pl.ds(chunk * CHUNK, CHUNK)
            target = pl.ds(chunk * half, half)
            parts = [
                part[:, source].astype(jnp.float32) * mix_gain_ref[:, source]
                for part in (query_ref, forget_ref, input_ref, gate_ref)
            ]
            parts.append(up_ref[source, :].astype(jnp.float32).T * ffn_gain_ref[:, source])
            rows = jnp.concatenate([part.astype(jnp.bfloat16) for part in parts], axis=0)
            rows = jnp.concatenate([rows, down_ref[:, source]], axis=0)
            picked = jnp.dot(rows, chosen, preferred_element_type=jnp.float32)
            picked = picked.astype(jnp.bfloat16)
            if own:
                mix_ref[:, target] = picked[:first]
                own_up_ref[:, target] = picked[first:second]
                own_down_ref[:, target] = picked[second:]
            else:
                other_ref[:first, target] = picked[:first]
                other_up_ref[:, target] = picked[first:second]
                other_down_ref[:, target] = picked[second:]
        start = pl.multiple_of(index * span, span)
        if own:
            own_out_ref[...] = out_ref[:, pl.ds(start, span)]
        else:
            for piece in range(2):
                other_ref[first:, pl.ds(piece * span, span)] = out_ref[
                    pl.ds(piece * lines, lines), pl.ds(start, span)
                ]


def split_weights(share, *operands):
    columns, hidden = operands[0].shape[0], operands[6].shape[0]
    lines, width = operands[4].shape[0], operands[0].shape[1] // 2
    core = lax.axis_index("tp").astype(jnp.int32).reshape(1)
    memory = pl.BlockSpec(memory_space=pltpu.VMEM)
    shapes = (
        (4 * columns, width),
        (hidden, width),
        (hidden, width),
        (lines, operands[4].shape[1] // 2),
        (4 * columns + lines // 2, width),
        (hidden, width),
        (hidden, width),
    )
    return pl.pallas_call(
        lambda *refs: split_kernel(share, *refs),
        out_shape=[jax.ShapeDtypeStruct(shape, jnp.bfloat16) for shape in shapes],
        in_specs=[pl.BlockSpec(memory_space=pltpu.SMEM)] + [memory] * len(operands),
        out_specs=[memory] * len(shapes),
    )(core, *operands)


def per_device(
    tokens,
    w_query,
    w_forget,
    w_input,
    w_output_gate,
    gate_floor,
    head_gain,
    w_out,
    mix_gain,
    ffn_gain,
    w_up,
    w_down,
    state,
):
    chips = lax.axis_size(KV)
    cores = lax.axis_size("tp")
    rows, share = tokens.shape
    width = chips * cores * share
    seq_local, heads_local, head_size, _ = state.shape
    tokens_t = tokens.T
    columns = w_query.shape[2]
    hidden_local = w_up.shape[1]

    tp = lax.axis_index("tp")

    token_half = gathered(tokens_t).reshape(chips * share, rows)
    own_mix, own_up, own_down, own_out, other, other_up, other_down = split_weights(
        share,
        *[w[:, 0, :].T for w in (w_query, w_forget, w_input, w_output_gate)],
        w_out.T,
        w_up,
        w_down,
        mix_gain[None, :],
        ffn_gain[None, :],
    )
    lent = swapped(other)
    first = 4 * columns
    span = lent.shape[1] // 2
    lent_out = jnp.concatenate([lent[first:, :span], lent[first:, span:]], axis=0)
    lent_mix, own_mix, own_out, lent_out = lax.optimization_barrier(
        (lent[:first], own_mix, own_out, lent_out)
    )
    lent_up, lent_down = swapped(other_up), swapped(other_down)
    sums = square_sums(token_half)
    high = sums.astype(jnp.bfloat16).astype(jnp.float32)
    place = lax.broadcasted_iota(jnp.int32, (128 - 4 * columns, rows), 0)
    extra = jnp.where(place == 0, high, jnp.where(place == 1, sums - high, 0.0))
    own = contracted(own_mix, token_half, (1, 0))
    theirs = contracted(lent_mix, token_half, (1, 0))
    first, second = jnp.where(tp == 0, own, theirs), jnp.where(tp == 0, theirs, own)
    raw = jnp.stack(
        [jnp.concatenate([part, extra], axis=0).T for part in (first, second)]
    ).astype(jnp.bfloat16)
    raw = raw.reshape(cores * chips, seq_local, 128)
    raw = lax.all_to_all(raw, ("tp", *KV), split_axis=0, concat_axis=0, tiled=True)
    raw, gate_floor, head_gain = lax.optimization_barrier((raw, gate_floor, head_gain))
    raw = raw.reshape(cores, chips, seq_local, 128).astype(jnp.float32).sum(axis=0)
    sums = raw[:1, :, 4 * columns : 4 * columns + 1] + raw[:1, :, 4 * columns + 1 : 4 * columns + 2]
    scale = lax.rsqrt(sums / width + EPSILON)
    raw = raw[:, :, : 4 * columns] * scale
    raw = raw.reshape(chips, seq_local, 4, columns).transpose(2, 1, 0, 3)
    raw = raw.reshape(4, seq_local, heads_local, head_size)
    raw = lax.optimization_barrier(raw)
    query_vec = raw[0] * head_size ** (-0.5)
    floor_heads = gate_floor.reshape(heads_local, head_size)
    forget_gate = floor_heads + (1.0 - floor_heads) * jax.nn.sigmoid(raw[1])
    input_vec = raw[2]
    gate_vec = raw[3]
    kept = jnp.sum((query_vec * forget_gate)[..., None] * state, axis=2)
    added = jnp.sum(query_vec * (1.0 - forget_gate), axis=-1, keepdims=True) * input_vec
    head_out = lax.optimization_barrier(kept) + added
    branch = rms_scale(head_out, head_gain) * jax.nn.silu(gate_vec)
    branch = branch.reshape(seq_local, heads_local * head_size).astype(jnp.bfloat16)

    branch, state, forget_gate, input_vec = lax.optimization_barrier(
        (branch, state, forget_gate, input_vec)
    )
    given = input_vec[:, :, None, :]
    new_state = given + forget_gate[..., None] * (state - given)

    branch_half = gathered(branch).reshape(rows, heads_local * head_size)
    theirs = swapped(contracted(lent_out, branch_half, (1, 1)))
    projected = contracted(own_out, branch_half, (1, 1)) + theirs
    residual = (tokens_t.astype(jnp.float32) + projected).astype(jnp.bfloat16)

    residual_half = gathered(residual).reshape(chips * share, rows)
    partial = jnp.concatenate(
        [contracted(up, residual_half, (1, 0)) for up in (own_up, lent_up)], axis=0
    )
    sums = square_sums(residual_half)
    arrived = swapped(jnp.concatenate([partial, sums], axis=0))
    upward = partial + jnp.concatenate(
        [arrived[hidden_local : 2 * hidden_local], arrived[:hidden_local]], axis=0
    )
    scale = lax.rsqrt((sums + arrived[-1:]) / width + EPSILON)
    hidden = jnp.square(jax.nn.relu(upward * scale)).astype(jnp.bfloat16)

    down_both = jnp.concatenate([own_down, lent_down], axis=0)
    terms = contracted(down_both, hidden, (0, 0)).astype(jnp.bfloat16)
    terms = lax.all_to_all(
        terms.reshape(chips, share, rows), KV, split_axis=0, concat_axis=0, tiled=True
    )
    summed = terms.astype(jnp.float32).sum(axis=0)
    mixed = (residual.astype(jnp.float32) + summed).astype(jnp.bfloat16).T
    return (mixed, new_state)


def solution(mesh):
    torus = Mesh(
        mesh.devices.reshape(mesh.shape["dp"], 8, 8, mesh.shape["tp"]), ("dp", "kv_0", "kv_1", "tp")
    )
    placed = (
        P("dp", KV_TP),
        P(None, "tp", KV),
        P(None, "tp", KV),
        P(None, "tp", KV),
        P(None, "tp", KV),
        P("tp"),
        P(),
        P(None, KV_TP),
        P(),
        P(),
        P(None, KV_TP),
        P(KV_TP, None),
        P(DP_KV, "tp", None, None),
    )

    return jax.shard_map(
        per_device,
        mesh=torus,
        in_specs=placed,
        out_specs=(P("dp", KV_TP), P(DP_KV, "tp", None, None)),
        check_vma=False,
    )
```
